128 devices in a mesh: sp: 16 (over z, y), dp: 8 (over x, core).
Axes of the slice: x: 4, y: 4, z: 4, core: 2. Of those that a mesh axis runs over, the one named last changes fastest.
Arguments:
- query_weight: bfloat16 [8, 6144, 1024], P('dp', 'sp'), may hold values from -6 to 6
- forget_preactivation: bfloat16 [8, 6144, 1024], P('dp', 'sp'), may hold values from -7 to 7
- written_input: bfloat16 [8, 6144, 1024], P('dp', 'sp'), may hold values from -6 to 6
- output_gate_logit: bfloat16 [8, 6144, 1024], P('dp', 'sp'), may hold values from -6 to 6
- forget_floor: float32 [1024], replicated, may hold values from 0.9 to 1
- extra_log_decay: float32 [8, 6144, 16], P('dp'), may hold values from -0.7 to 0
- residual: bfloat16 [8, 6144, 2048], P('dp', 'sp'), may hold values from -6 to 6
- output_weight: bfloat16 [1024, 2048], P('dp'), may hold values from -0.1875 to 0.1875
- norm_scale_vector: float32 [2048], replicated, may hold values from 0.1 to 1.9
- expert_gate_weight: bfloat16 [16, 2048, 1024], P('sp'), may hold values from -0.125 to 0.125
- expert_up_weight: bfloat16 [16, 2048, 1024], P('sp'), may hold values from -0.125 to 0.125
- expert_down_weight: bfloat16 [16, 1024, 2048], P('sp'), may hold values from -0.1875 to 0.1875
- routes: int32 [8, 6144, 2], P('dp', 'sp'), may hold values from 0 to 15, as said below
- routing_weight: float32 [8, 6144, 2], P('dp', 'sp'), may hold values from 0.2 to 1
Outputs:
- layer_out: bfloat16 [8, 6144, 2048], P('dp', 'sp')
The draws below stay inside these ranges and needn't reach their ends.
Inputs may be any that keep to these rules, and one draw needn't show every extreme that they name: `routes`: the two experts of a position differ and lie in one group of four, 4 g to 4 g + 3. In the positions of one device no expert is named more than 96 times. In every draw one expert is named exactly 96 times by the positions of every device, and on some devices each of the four experts of one group is named exactly 96 times.
All inputs are finite; a program needn't handle non-finite values.
Results may differ from the reference program's by a relative error of at most 0.0059.
Values may be sent and summed in bfloat16 or wider, within the bound.
No kernel may reach another device: no remote copies, remote signals or barrier semaphores. Data moves between devices by JAX's collectives and lax.ppermute only.
A program may use at most 128 MiB of HBM per device.

```python
import math
import jax
import jax.numpy as jnp
from jax import lax

D = 2048
RECURRENT_HEADS = 16
HEAD_CHANNELS = 64
W = 1024
DE = 1024
BLOCK = 64
TOK_DEV = 384
SEQS = 8
LEN = 6144
EXPERTS = 16
GROUPS = 4
CAP = 96
N_SP = 16


def draw_forget_preactivation(key, part):
    subkeys = jax.random.split(jax.random.fold_in(key, 3), 2)
    jitter = jnp.clip(jax.random.normal(subkeys[0], (SEQS, LEN, RECURRENT_HEADS, HEAD_CHANNELS), jnp.float32), -5.0, 5.0)
    shards = LEN // TOK_DEV
    shifts = jax.random.uniform(subkeys[1], (SEQS, shards, 1, RECURRENT_HEADS, 1), jnp.float32, -1.2, 1.2)
    values = jitter.reshape(SEQS, shards, TOK_DEV, RECURRENT_HEADS, HEAD_CHANNELS) + shifts
    return values.reshape(SEQS, LEN, W).astype(jnp.bfloat16)


def draw_forget_floor(key, part):
    subkeys = jax.random.split(jax.random.fold_in(key, 5), 4)
    share = 0.5
    slow = jax.random.bernoulli(subkeys[0], share, (RECURRENT_HEADS, 1))
    slow_rate = jnp.exp(jax.random.uniform(subkeys[1], (RECURRENT_HEADS, 1), jnp.float32, math.log(0.15), math.log(1.2))) / LEN
    fast_rate = jnp.exp(jax.random.uniform(subkeys[2], (RECURRENT_HEADS, 1), jnp.float32, math.log(0.04), math.log(0.1)))
    channel = jnp.exp(jax.random.uniform(subkeys[3], (RECURRENT_HEADS, HEAD_CHANNELS), jnp.float32, math.log(0.5), 0.0))
    rates = jnp.where(slow, slow_rate, fast_rate) * channel
    return (1.0 - rates).reshape(W).astype(jnp.float32)


def draw_extra_log_decay(key, part):
    subkeys = jax.random.split(jax.random.fold_in(key, 9), 2)
    places = jax.random.randint(subkeys[0], (SEQS, 3), 0, LEN)
    depth = jnp.log(jax.random.uniform(subkeys[1], (SEQS, 3, RECURRENT_HEADS), jnp.float32, 0.5, 0.8))
    marks = (jnp.arange(LEN)[None, :, None] == places[:, None, :]).astype(jnp.float32)
    return jnp.einsum('slb,sbh->slh', marks, depth).astype(jnp.float32)


def draw_routes(key, part):
    blocks_all = SEQS * LEN // TOK_DEV
    others = GROUPS - 1
    subkeys = jax.random.split(jax.random.fold_in(key, 13), 9)
    busiest = jax.random.randint(subkeys[0], (), 0, EXPERTS)
    hot_group = busiest // 4
    hot_local = busiest % 4
    spread = jax.random.randint(subkeys[1], (blocks_all, others), 0, CAP // 4 + 1)
    counts = CAP + spread - jnp.roll(spread, -1, axis=1)
    group_ends = jnp.cumsum(counts, axis=1)
    rotate = jax.random.randint(subkeys[2], (blocks_all, 1), 0, others)
    offset = jax.random.randint(subkeys[3], (blocks_all, GROUPS), 0, 4)
    places = jnp.broadcast_to(jnp.arange(TOK_DEV)[None, :], (blocks_all, TOK_DEV))
    remain = places - CAP
    slot_group = jnp.sum((remain[:, :, None] >= group_ends[:, None, :]).astype(jnp.int32), axis=2)
    slot_group = jnp.minimum(slot_group, others - 1)
    group_starts = jnp.take_along_axis(group_ends - counts, slot_group, axis=1)
    inside = remain - group_starts
    other_group = (hot_group + 1 + (slot_group + rotate) % others) % GROUPS
    shift_by = jnp.take_along_axis(offset, other_group, axis=1)
    primary_other = other_group * 4 + (inside + shift_by) % 4
    secondary_other = other_group * 4 + (inside + shift_by + 1) % 4
    secondary_hot = hot_group * 4 + (hot_local + 1 + places % 3) % 4
    is_hot = places < CAP
    drawn_primary = jnp.where(is_hot, busiest, primary_other)
    drawn_secondary = jnp.where(is_hot, secondary_hot, secondary_other)
    matching = jax.random.randint(subkeys[6], (blocks_all,), 0, 3)
    table = jnp.array([[0, 1, 2, 3], [0, 2, 1, 3], [0, 3, 1, 2]], jnp.int32)
    pairing = table[matching]
    parity = places % 2
    first_local = jnp.take_along_axis(pairing, 2 * parity, axis=1)
    second_local = jnp.take_along_axis(pairing, 2 * parity + 1, axis=1)
    leftover = jnp.maximum(places - 2 * CAP, 0)
    leftover_group = (hot_group + 1 + (leftover + rotate) % others) % GROUPS
    leftover_shift = jnp.take_along_axis(offset, leftover_group, axis=1)
    within = leftover // others
    in_full = places < 2 * CAP
    full_primary = jnp.where(in_full, hot_group * 4 + first_local, leftover_group * 4 + (within + leftover_shift) % 4)
    full_secondary = jnp.where(in_full, hot_group * 4 + second_local, leftover_group * 4 + (within + leftover_shift + 1) % 4)
    chosen = jax.random.randint(subkeys[7], (blocks_all, 1), 0, 2)
    forced = jax.random.randint(subkeys[8], (), 0, blocks_all)
    block_index = jnp.arange(blocks_all, dtype=jnp.int32)[:, None]
    full_block = jnp.where(block_index == forced, 1, jnp.where(block_index == (forced + 1) % blocks_all, 0, chosen))
    primary = jnp.where(full_block == 1, full_primary, drawn_primary)
    secondary = jnp.where(full_block == 1, full_secondary, drawn_secondary)
    scores = jax.random.randint(subkeys[4], (blocks_all, TOK_DEV), 0, TOK_DEV) * TOK_DEV + places
    shuffle = jnp.argsort(scores, axis=1)
    primary = jnp.take_along_axis(primary, shuffle, axis=1)
    secondary = jnp.take_along_axis(secondary, shuffle, axis=1)
    flipped = jax.random.randint(subkeys[5], (blocks_all, TOK_DEV, 1), 0, 2)
    straight = jnp.stack([primary, secondary], axis=2)
    crossed = jnp.stack([secondary, primary], axis=2)
    paired = jnp.where(flipped == 1, crossed, straight)
    return paired.reshape(SEQS, LEN, 2).astype(jnp.int32)


def levels(rng, dims, cuts, low, largest):
    level = 1.0
    for dim, blocks in cuts:
        heights = jax.random.uniform(jax.random.fold_in(jax.random.fold_in(rng, 6), dim), (blocks,), jnp.float32, low / len(cuts), largest / len(cuts))
        level = level * jnp.repeat(jnp.exp(heights), dims[dim] // blocks).reshape((-1,) + (1,) * (len(dims) - 1 - dim))
    return level


def scatter_about(key, shape, deviation, limit, pieces=(), held_as=jnp.bfloat16):
    gain = levels(key, shape, pieces, -0.22, 0.18) if pieces else 1.0
    values = jax.random.normal(key, shape, jnp.float32) * deviation * gain
    return jnp.minimum(jnp.maximum(values, -limit), limit).astype(held_as)


def setup_inputs(seed: int = 0) -> dict:
    seeds = jax.random.split(jax.random.key(seed), 15)
    return {
        "query_weight": scatter_about(seeds[0], (SEQS, LEN, W), 1.0, 6.0, ((0, 8), (1, 16))),
        "forget_preactivation": draw_forget_preactivation(jax.random.fold_in(seeds[14], 71), 0),
        "written_input": scatter_about(seeds[2], (SEQS, LEN, W), 1.0, 6.0, ((0, 8), (1, 16))),
        "output_gate_logit": scatter_about(seeds[3], (SEQS, LEN, W), 1.0, 6.0, ((0, 8), (1, 16))),
        "forget_floor": draw_forget_floor(jax.random.fold_in(seeds[14], 71), 0),
        "extra_log_decay": draw_extra_log_decay(jax.random.fold_in(seeds[14], 71), 0),
        "residual": scatter_about(seeds[6], (SEQS, LEN, D), 1.0, 6.0, ((0, 8), (1, 16))),
        "output_weight": scatter_about(seeds[7], (W, D), W ** -0.5, 0.1875, ((0, 8),)),
        "norm_scale_vector": jnp.clip(1.0 + 0.18 * jax.random.normal(seeds[8], (D,), jnp.float32), 0.1, 1.9),
        "expert_gate_weight": scatter_about(seeds[9], (EXPERTS, D, DE), D ** -0.5, 0.125, ((0, 16),)),
        "expert_up_weight": scatter_about(seeds[10], (EXPERTS, D, DE), D ** -0.5, 0.125, ((0, 16),)),
        "expert_down_weight": scatter_about(seeds[11], (EXPERTS, DE, D), DE ** -0.5, 0.1875, ((0, 16),)),
        "routes": draw_routes(jax.random.fold_in(seeds[14], 71), 0),
        "routing_weight": jnp.clip(0.2 + 0.8 * jax.random.uniform(seeds[13], (SEQS, LEN, 2), jnp.float32) ** levels(seeds[13], (SEQS, LEN, 2), ((0, 8), (1, 16)), -0.2, 0.2), 0.2, 1.0),
    }


HIGHEST = lax.Precision.HIGHEST

def head_norm(values):
    return values * lax.rsqrt(lax.optimization_barrier(jnp.mean(values * values, axis=-1, keepdims=True)) + 1e-06)

def linear_recurrent(query_unprojected, forget_unbounded, value_unprojected, floor_level, decay_spikes, prefixed_state):
    seq_count, length, head_count, channels = query_unprojected.shape
    block_count = length // BLOCK
    queries = jax.nn.silu(query_unprojected)
    forget_logarithm = jnp.logaddexp(jnp.log(floor_level), jnp.log1p(-floor_level) + jax.nn.log_sigmoid(forget_unbounded)) + decay_spikes[..., None]
    keys_in = (1.0 - floor_level) * jax.nn.sigmoid(-forget_unbounded)

    def to_blocks(tensor):
        return tensor.reshape(seq_count, block_count, BLOCK, head_count, channels).transpose(1, 0, 3, 2, 4)
    q_blocks = to_blocks(queries)
    k_blocks = to_blocks(keys_in)
    v_blocks = to_blocks(value_unprojected)
    cumulative = jnp.cumsum(to_blocks(forget_logarithm), axis=3)
    causal = jnp.tril(jnp.ones((BLOCK, BLOCK), bool))[:, :, None]

    def advance(states, inputs):
        block_q, block_k, block_v, block_b = inputs
        spread_log = block_b[:, :, :, None, :] - block_b[:, :, None, :, :]
        decays = jnp.where(causal, jnp.exp(jnp.where(causal, spread_log, 0.0)), 0.0)
        scores = jnp.einsum('bhtk,bhsk,bhtsk->bhts', block_q, block_k, decays, precision=HIGHEST)
        outputs = jnp.einsum('bhts,bhsv->bhtv', scores, block_v, precision=HIGHEST)
        outputs = outputs + jnp.einsum('bhtk,bhkv->bhtv', block_q * jnp.exp(block_b), states, precision=HIGHEST)
        closing = block_b[:, :, -1:, :]
        states = jnp.exp(closing[:, :, 0, :, None]) * states + jnp.einsum('bhsk,bhsv->bhkv', block_k * jnp.exp(closing - block_b), block_v, precision=HIGHEST)
        return (states, outputs)
    initial = jnp.zeros((seq_count, head_count, channels, channels), jnp.float32)
    states, outputs = lax.scan(advance, initial, (q_blocks, k_blocks, v_blocks, cumulative))
    final_output = outputs.transpose(1, 0, 3, 2, 4).reshape(seq_count, length, head_count, channels)
    if prefixed_state:
        totals = cumulative[:, :, :, -1, :]
        before = jnp.cumsum(totals, axis=0) - totals
        running = (cumulative + before[:, :, :, None, :]).transpose(1, 0, 3, 2, 4)
        running = running.reshape(seq_count, length, head_count, channels)
        return (final_output, states, running, queries)
    return (final_output, states, None, queries)

def reference(query_weight, forget_preactivation, written_input, output_gate_logit, forget_floor, extra_log_decay, residual, output_weight, norm_scale_vector, expert_gate_weight, expert_up_weight, expert_down_weight, routes, routing_weight):

    def divide_into_heads(tensor):
        return tensor.astype(jnp.float32).reshape(SEQS, LEN, RECURRENT_HEADS, HEAD_CHANNELS)
    final_output, unused_item, unused_item, unused_item = linear_recurrent(divide_into_heads(query_weight), divide_into_heads(forget_preactivation), divide_into_heads(written_input), forget_floor.reshape(RECURRENT_HEADS, HEAD_CHANNELS), extra_log_decay, False)
    mixer_out = (head_norm(final_output) * jax.nn.silu(divide_into_heads(output_gate_logit))).astype(jnp.bfloat16)
    total_rows = SEQS * LEN
    mixer_out = mixer_out.reshape(total_rows, W)
    updated = (residual.reshape(total_rows, D).astype(jnp.float32) + jnp.dot(mixer_out, output_weight, preferred_element_type=jnp.float32)).astype(jnp.bfloat16)
    widened = lax.optimization_barrier(updated).astype(jnp.float32)
    normed = (widened * lax.rsqrt(lax.optimization_barrier(jnp.mean(widened * widened, axis=-1, keepdims=True)) + 1e-06) * norm_scale_vector.astype(jnp.float32)).astype(jnp.bfloat16)
    padded = jnp.concatenate([normed, jnp.zeros((1, D), jnp.bfloat16)], axis=0)
    picks = jnp.concatenate([routes.reshape(-1), jnp.full((1,), -1, jnp.int32)])
    weights = jnp.concatenate([routing_weight.reshape(-1), jnp.zeros((1,), jnp.float32)])
    bound_rows = SEQS * N_SP * CAP

    def serve(summed, expert):
        found = jnp.nonzero(picks == expert, size=bound_rows, fill_value=2 * total_rows)[0].astype(jnp.int32)
        tokens_hit = found // 2
        picked = padded[tokens_hit]
        gated = jnp.dot(picked, expert_gate_weight[expert], preferred_element_type=jnp.float32)
        upward = jnp.dot(picked, expert_up_weight[expert], preferred_element_type=jnp.float32)
        hidden = (jax.nn.silu(gated) * upward).astype(jnp.bfloat16)
        produced = jnp.dot(hidden, expert_down_weight[expert], preferred_element_type=jnp.float32).astype(jnp.bfloat16)
        produced = lax.optimization_barrier(produced).astype(jnp.float32)
        summed = summed.at[tokens_hit].add(weights[found][:, None] * produced)
        return (summed, None)
    summed, unused_item = lax.scan(serve, jnp.zeros((total_rows + 1, D), jnp.float32), jnp.arange(EXPERTS, dtype=jnp.int32))
    layer_out = (widened + summed[:total_rows]).astype(jnp.bfloat16)
    return layer_out.reshape(SEQS, LEN, D)
```

```python
import functools

import jax
import jax.numpy as jnp
from jax import lax
from jax.experimental import pallas as pl
from jax.experimental.pallas import tpu as pltpu
from jax.sharding import Mesh
from jax.sharding import PartitionSpec as P

CH = 64
BLK = 64
GL = 256
SP = ("sp_0", "sp_1")
DP = ("x", "c")
PACK = 80
F32 = jnp.float32
BF = jnp.bfloat16


def dot(a, b, dims=((1,), (0,))):
    return lax.dot_general(a, b, (dims, ((), ())), preferred_element_type=F32)


def split3(v):
    hi = v.astype(BF)
    rest = v - hi.astype(F32)
    mid = rest.astype(BF)
    low = (rest - mid.astype(F32)).astype(BF)
    return hi, mid, low


def split2(v):
    hi = v.astype(BF)
    return hi, (v - hi.astype(F32)).astype(BF)


def tri(n):
    return (
        lax.broadcasted_iota(jnp.int32, (n, n), 0) >= lax.broadcasted_iota(jnp.int32, (n, n), 1)
    )


def same_head(rows, lanes):
    return (
        lax.broadcasted_iota(jnp.int32, (rows, lanes), 0) // CH
        == lax.broadcasted_iota(jnp.int32, (rows, lanes), 1) // CH
    )


def silu(v):
    return v / (1.0 + jnp.exp(-v))


def keys_and_logs(f_ref, floor_ref, spike_ref, group):
    f = f_ref[...].astype(F32)
    keys = (1.0 - floor_ref[...]) / (1.0 + jnp.exp(f))
    poly = jnp.full_like(keys, 1.0 / 10.0)
    for n in range(9, 0, -1):
        poly = poly * keys + 1.0 / n
    heads = spike_ref.shape[1]
    spread = (
        lax.broadcasted_iota(jnp.int32, (heads, GL), 0)
        == group * (GL // CH) + lax.broadcasted_iota(jnp.int32, (heads, GL), 1) // CH
    ).astype(BF)
    hi, mid, low = split3(spike_ref[...])
    burst = dot(hi, spread) + dot(mid, spread) + dot(low, spread)
    return keys, burst - keys * poly


def running_sum(logs, length):
    lower = tri(length).astype(BF)
    out = []
    for b in range(logs.shape[0] // length):
        hi, mid, low = split3(logs[b * length : (b + 1) * length])
        out.append(dot(lower, hi) + dot(lower, mid) + dot(lower, low))
    return out


def states_kernel(f_ref, v_ref, floor_ref, spike_ref, pack_ref):
    group = pl.program_id(0)
    keys, logs = keys_and_logs(f_ref, floor_ref, spike_ref, group)
    parts = running_sum(logs, 128)
    after = jnp.zeros((1, GL), F32)
    acc = jnp.zeros((GL, GL), F32)
    for b in reversed(range(len(parts))):
        close = parts[b][127:128]
        kc = (keys[b * 128 : (b + 1) * 128] * jnp.exp(after + close - parts[b])).astype(BF)
        acc = acc + dot(v_ref[b * 128 : (b + 1) * 128, :], kc, ((0,), (0,)))
        after = after + close
    acc = jnp.where(same_head(GL, GL), acc, 0.0)
    compact = acc[0:64] + acc[64:128] + acc[128:192] + acc[192:256]
    pack_ref[0:64, :] = compact.astype(BF)
    hi, mid, low = split3(after)
    row = lax.broadcasted_iota(jnp.int32, (16, GL), 0)
    tail = jnp.where(row == 0, hi.astype(F32), 0.0)
    tail = jnp.where(row == 1, mid.astype(F32), tail)
    tail = jnp.where(row == 2, low.astype(F32), tail)
    pack_ref[64:80, :] = tail.astype(BF)


def inside_kernel(q_ref, f_ref, v_ref, floor_ref, spike_ref, out_ref, qrun_ref):
    group = pl.program_id(0)
    keys, logs = keys_and_logs(f_ref, floor_ref, spike_ref, group)
    parts = running_sum(logs, BLK)
    q = silu(q_ref[...].astype(F32))
    head_mask = same_head(GL, GL)
    lane = lax.broadcasted_iota(jnp.int32, (BLK, GL), 1)
    causal = (lane % CH) <= lax.broadcasted_iota(jnp.int32, (BLK, GL), 0)
    before = jnp.zeros((1, GL), F32)
    state = jnp.zeros((GL, GL), F32)
    zero = jnp.zeros((GL, GL), BF)
    for b in range(len(parts)):
        rows = slice(b * BLK, (b + 1) * BLK)
        cum = parts[b]
        close = cum[BLK - 1 : BLK]
        k = keys[rows]
        grow = jnp.exp(-cum)
        qd = q[rows] * jnp.exp(cum)
        qrun_ref[rows, :] = (qd * jnp.exp(before)).astype(BF)
        qd = qd.astype(BF)
        kg = (k * grow).astype(BF)
        v = v_ref[rows, :]
        k4 = jnp.where(head_mask, jnp.concatenate([kg] * 4, axis=0), zero)
        v4 = jnp.where(head_mask, jnp.concatenate([v] * 4, axis=0), zero)
        scores = dot(qd, k4, ((1,), (1,)))
        scores = jnp.where(causal, scores, 0.0).astype(BF)
        out = dot(scores, v4)
        if b > 0:
            out = out + dot(qd, state.astype(BF), ((1,), (1,)))
        out_ref[rows, :] = out
        if b + 1 < len(parts):
            kc = (k * jnp.exp(close - cum)).astype(BF)
            add = jnp.where(head_mask, dot(v, kc, ((0,), (0,))), 0.0)
            state = jnp.exp(close) * state + add
        before = before + close


def total_of(pack_ref):
    return (
        pack_ref[64:65, :].astype(F32)
        + pack_ref[65:66, :].astype(F32)
        + pack_ref[66:67, :].astype(F32)
    )


def row_kernel(pos_ref, own_ref, one_ref, two_ref, three_ref, row_ref, before_ref, btot_ref):
    here = pos_ref[0]
    width = own_ref.shape[1]
    state = jnp.zeros((CH, width), F32)
    total = jnp.zeros((1, width), F32)
    pieces = ((3, three_ref), (2, two_ref), (1, one_ref))
    for n, ref in pieces:
        use = n <= here
        t = jnp.where(use, total_of(ref), 0.0)
        state = jnp.exp(t) * state + jnp.where(use, ref[0:64, :].astype(F32), 0.0)
        total = total + t
    before_ref[...] = state
    btot_ref[...] = jnp.broadcast_to(total, (8, width))
    t = total_of(own_ref)
    state = jnp.exp(t) * state + own_ref[0:64, :].astype(F32)
    total = total + t
    for n, ref in pieces:
        use = n > here
        t = jnp.where(use, total_of(ref), 0.0)
        state = jnp.exp(t) * state + jnp.where(use, ref[0:64, :].astype(F32), 0.0)
        total = total + t
    row_ref[0:64, :] = state.astype(BF)
    hi, mid, low = split3(total)
    row = lax.broadcasted_iota(jnp.int32, (16, width), 0)
    tail = jnp.where(row == 0, hi.astype(F32), 0.0)
    tail = jnp.where(row == 1, mid.astype(F32), tail)
    tail = jnp.where(row == 2, low.astype(F32), tail)
    row_ref[64:80, :] = tail.astype(BF)


def mix_kernel(
    tok_steps,
    half,
    pos_ref,
    out_ref,
    qrun_ref,
    gate_ref,
    res_ref,
    before_ref,
    btot_ref,
    one_ref,
    two_ref,
    three_ref,
    wmine_ref,
    wother_ref,
    scale_ref,
    routes_ref,
    upd_ref,
    send_a_ref,
    send_b_ref,
    w_s,
    state_s,
    norm_s,
    pos_s,
    mem_s,
):
    step = pl.program_id(0)
    width = gate_ref.shape[1]
    groups = width // GL
    tok_rows = routes_ref.shape[1]
    rows = gate_ref.shape[0]

    @pl.when(step == 0)
    def _():
        here = pos_ref[0]
        state = jnp.zeros((CH, width), F32)
        for n, ref in ((3, three_ref), (2, two_ref), (1, one_ref)):
            use = n <= here
            t = jnp.where(use, total_of(ref), 0.0)
            state = jnp.exp(t) * state + jnp.where(use, ref[0:64, :].astype(F32), 0.0)
        state = (jnp.exp(btot_ref[0:1, :]) * state + before_ref[...]).astype(BF)
        mask = same_head(GL, GL)
        for g in range(groups):
            one = state[:, g * GL : (g + 1) * GL]
            state_s[g] = jnp.where(mask, jnp.concatenate([one] * 4, axis=0), jnp.zeros((GL, GL), BF))
        x_here = pos_ref[1]
        core = pos_ref[2]
        piece = wmine_ref.shape[1]
        for n in range(4):
            src = (x_here + 4 - n) % 4
            w_s[pl.ds((2 * src + core) * piece, piece), :] = wmine_ref[n]
            w_s[pl.ds((2 * src + 1 - core) * piece, piece), :] = wother_ref[n]
        experts = mem_s.shape[0]
        e = lax.broadcasted_iota(jnp.int32, (experts, tok_rows), 0)
        member = (e == routes_ref[0:1, :]) | (e == routes_ref[1:2, :])
        mem = jnp.where(member, 1.0, 0.0)
        strict = (
            lax.broadcasted_iota(jnp.int32, (tok_rows, tok_rows), 0)
            < lax.broadcasted_iota(jnp.int32, (tok_rows, tok_rows), 1)
        ).astype(BF)
        place = dot(mem.astype(BF), strict)
        pos_s[...] = jnp.where(member, place.astype(jnp.int32), -1)

    @pl.when(step < tok_steps)
    def _():
        ones = jnp.where(same_head(GL, GL), 1.0, 0.0).astype(BF)
        mixed = []
        for g in range(groups):
            lanes = slice(g * GL, (g + 1) * GL)
            o = out_ref[:, lanes] + dot(qrun_ref[:, lanes], state_s[g], ((1,), (1,)))
            hi, low = split2(o * o)
            mean = (dot(hi, ones) + dot(low, ones)) * (1.0 / CH)
            gate = silu(gate_ref[:, lanes].astype(F32))
            mixed.append((o * lax.rsqrt(mean + 1e-06) * gate).astype(BF))
        mixed = jnp.concatenate(mixed, axis=1)
        upd = (res_ref[...].astype(F32) + dot(mixed, w_s[...])).astype(BF)
        upd_ref[...] = upd
        wide = upd.astype(F32)
        mean = jnp.mean(wide * wide, axis=-1, keepdims=True)
        norm = (wide * lax.rsqrt(mean + 1e-06) * scale_ref[...]).astype(BF)
        norm_s[pl.ds(step * rows, rows), :] = norm

    def send(ref, first, base):
        picks = []
        for i in range(ref.shape[0] // half):
            place = pos_s[pl.ds(first + i, 1), :]
            c = lax.broadcasted_iota(jnp.int32, (half, tok_rows), 0) + base
            picks.append(jnp.where(c == place, 1.0, 0.0).astype(BF))
        ref[...] = dot(jnp.concatenate(picks, axis=0), norm_s[...]).astype(BF)

    per = send_a_ref.shape[0] // half
    blocks = mem_s.shape[0] // per

    @pl.when((step >= tok_steps) & (step < tok_steps + blocks))
    def _():
        send(send_a_ref, (step - tok_steps) * per, 0)

    @pl.when(step >= tok_steps + blocks)
    def _():
        send(send_b_ref, (step - tok_steps - blocks) * per, half)


def combine_kernel(cap, half, base, last, routes_ref, wt_ref, got_ref, acc_ref, out_ref, hi_s, low_s):
    experts = got_ref.shape[0] // half
    tok_rows = routes_ref.shape[0]

    @pl.when(pl.program_id(0) == 0)
    def _():
        lane = lax.broadcasted_iota(jnp.int32, (tok_rows, 128), 1)
        r0 = routes_ref[:, 0:1]
        r1 = routes_ref[:, 1:2]
        oh0 = lane == r0
        oh1 = lane == r1
        mem = jnp.where(oh0 | oh1, 1.0, 0.0).astype(BF)
        strict = (
            lax.broadcasted_iota(jnp.int32, (tok_rows, tok_rows), 0)
            > lax.broadcasted_iota(jnp.int32, (tok_rows, tok_rows), 1)
        ).astype(BF)
        place = dot(strict, mem)
        j = lax.broadcasted_iota(jnp.int32, (tok_rows, experts * half), 1)
        weight = jnp.zeros((tok_rows, experts * half), F32)
        for k, (oh, r) in enumerate(((oh0, r0), (oh1, r1))):
            p = jnp.sum(jnp.where(oh, place, 0.0), axis=1, keepdims=True).astype(jnp.int32) - base
            slot = jnp.where((p >= 0) & (p < half), r * half + p, -1)
            weight = weight + jnp.where(j == slot, wt_ref[:, k : k + 1], 0.0)
        hi, low = split2(weight)
        hi_s[...] = hi
        low_s[...] = low

    got = got_ref[...]
    total = acc_ref[...].astype(F32) + (dot(hi_s[...], got) + dot(low_s[...], got))
    out_ref[...] = total.astype(out_ref.dtype)


def ring(n, size=4):
    return [(i, (i + n) % size) for i in range(size)]


def per_device(
    query_weight,
    forget_preactivation,
    written_input,
    output_gate_logit,
    forget_floor,
    extra_log_decay,
    residual,
    output_weight,
    norm_scale_vector,
    expert_gate_weight,
    expert_up_weight,
    expert_down_weight,
    routes,
    routing_weight,
):
    _, tok, width = query_weight.shape
    model = output_weight.shape[1]
    piece = output_weight.shape[0]
    heads = width // CH
    groups = width // GL
    experts = lax.axis_size(SP)
    cap = 4 * tok // experts
    half = cap // 2
    z = lax.axis_index("sp_0")
    y = lax.axis_index("sp_1")
    x = lax.axis_index("x")
    core = lax.axis_index("c")

    spikes = lax.dynamic_slice_in_dim(extra_log_decay[0], lax.axis_index(SP) * tok, tok, 0)
    q, f, v, gate = (
        a.reshape(tok, width)
        for a in (query_weight, forget_preactivation, written_input, output_gate_logit)
    )
    floor = forget_floor.reshape(1, width)
    scale = norm_scale_vector.reshape(1, model)
    res = residual.reshape(tok, model)

    wpieces = [output_weight] + [lax.ppermute(output_weight, "x", ring(n)) for n in (1, 2, 3)]

    tall = pl.BlockSpec((tok, GL), lambda g: (0, g))
    flat = pl.BlockSpec((1, GL), lambda g: (0, g))
    whole = pl.BlockSpec((tok, heads), lambda g: (0, 0))
    pack = pl.pallas_call(
        states_kernel,
        grid=(groups,),
        in_specs=[tall, tall, flat, whole],
        out_specs=pl.BlockSpec((PACK, GL), lambda g: (0, g)),
        out_shape=jax.ShapeDtypeStruct((PACK, width), BF),
        name="states",
    )(f, v, floor, spikes)

    along_y = [lax.ppermute(pack, "sp_1", ring(n)) for n in (1, 2, 3)]

    inside, qrun = pl.pallas_call(
        inside_kernel,
        grid=(groups,),
        in_specs=[tall, tall, tall, flat, whole],
        out_specs=[tall, tall],
        out_shape=[
            jax.ShapeDtypeStruct((tok, width), F32),
            jax.ShapeDtypeStruct((tok, width), BF),
        ],
        name="inside",
    )(q, f, v, floor, spikes)

    vm = pl.BlockSpec(memory_space=pltpu.VMEM)
    sm = pl.BlockSpec(memory_space=pltpu.SMEM)
    row, before, btot = pl.pallas_call(
        row_kernel,
        in_specs=[sm, vm, vm, vm, vm],
        out_specs=[vm, vm, vm],
        out_shape=[
            jax.ShapeDtypeStruct((PACK, width), BF),
            jax.ShapeDtypeStruct((CH, width), F32),
            jax.ShapeDtypeStruct((8, width), F32),
        ],
        name="row",
    )(y.astype(jnp.int32).reshape(1), pack, *along_y)

    along_z = [lax.ppermute(row, "sp_0", ring(n)) for n in (1, 2, 3)]

    wmine = jnp.stack(wpieces)
    wother = lax.ppermute(wmine, "c", [(0, 1), (1, 0)])

    route_rows = jnp.pad(routes[0].T, ((0, 6), (0, 0)), constant_values=-1)
    place = jnp.stack([z, x, core]).astype(jnp.int32)
    tok_steps = 3
    rows = tok // tok_steps
    send_steps = 4
    send_rows = 2 * experts * half // send_steps
    clip = lambda i: jnp.minimum(i, tok_steps - 1)
    tok_w = pl.BlockSpec((rows, width), lambda i: (clip(i), 0))
    tok_m = pl.BlockSpec((rows, model), lambda i: (clip(i), 0))
    full = lambda a: pl.BlockSpec(a.shape, lambda i: (0,) * a.ndim)


    updated, send_a, send_b = pl.pallas_call(
        functools.partial(mix_kernel, tok_steps, half),
        grid=(tok_steps + send_steps,),
        in_specs=[
            sm,
            tok_w,
            tok_w,
            tok_w,
            tok_m,
            full(before),
            full(btot),
            full(row),
            full(row),
            full(row),
            full(wmine),
            full(wmine),
            full(scale),
            full(route_rows),
        ],
        out_specs=[
            tok_m,
            pl.BlockSpec((send_rows, model), lambda i: (jnp.clip(i - tok_steps, 0, 1), 0)),
            pl.BlockSpec((send_rows, model), lambda i: (jnp.clip(i - tok_steps - 2, 0, 1), 0)),
        ],
        out_shape=[
            jax.ShapeDtypeStruct((tok, model), BF),
            jax.ShapeDtypeStruct((experts * half, model), BF),
            jax.ShapeDtypeStruct((experts * half, model), BF),
        ],
        scratch_shapes=[
            pltpu.VMEM((width, model), BF),
            pltpu.VMEM((groups, GL, GL), BF),
            pltpu.VMEM((tok, model), BF),
            pltpu.VMEM((experts, tok), jnp.int32),
            pltpu.VMEM((experts, tok), jnp.int32),
        ],
        compiler_params=pltpu.CompilerParams(vmem_limit_bytes=50 * 1024 * 1024),
        name="mix",
    )(place, inside, qrun, gate, res, before, btot, *along_z, wmine, wother, scale, route_rows)

    def exchange(a):
        return lax.all_to_all(
            a.reshape(experts, half, model), SP, split_axis=0, concat_axis=0, tiled=True
        ).reshape(experts * half, model)

    def serve(a):
        gated = jnp.dot(a, expert_gate_weight[0], preferred_element_type=F32)
        upward = jnp.dot(a, expert_up_weight[0], preferred_element_type=F32)
        hidden = (jax.nn.silu(gated) * upward).astype(BF)
        return jnp.dot(hidden, expert_down_weight[0], preferred_element_type=F32).astype(BF)

    def combine(got, acc, base, last):
        blk = 512
        return pl.pallas_call(
            functools.partial(combine_kernel, cap, half, base, last),
            grid=(model // blk,),
            in_specs=[
                pl.BlockSpec((tok, 2), lambda i: (0, 0)),
                pl.BlockSpec((tok, 2), lambda i: (0, 0)),
                pl.BlockSpec((experts * half, blk), lambda i: (0, i)),
                pl.BlockSpec((tok, blk), lambda i: (0, i)),
            ],
            out_specs=pl.BlockSpec((tok, blk), lambda i: (0, i)),
            out_shape=jax.ShapeDtypeStruct((tok, model), BF if last else F32),
            scratch_shapes=[pltpu.VMEM((tok, experts * half), BF)] * 2,
            name="combine",
        )(routes[0], routing_weight[0], got, acc)

    in_a = exchange(send_a)
    in_b = exchange(send_b)
    got_a = exchange(serve(in_a))
    got_b = exchange(serve(in_b))
    acc = combine(got_a, updated, 0, False)
    layer_out = combine(got_b, acc, half, True)
    return layer_out.reshape(1, tok, model)


def solution(mesh):
    torus = Mesh(
        mesh.devices.reshape(4, 4, 4, mesh.shape["dp"] // 4), ("sp_0", "sp_1", "x", "c")
    )
    return jax.shard_map(
        per_device,
        mesh=torus,
        in_specs=(
            P(DP, SP, None),
            P(DP, SP, None),
            P(DP, SP, None),
            P(DP, SP, None),
            P(),
            P(DP, None, None),
            P(DP, SP, None),
            P(DP, None),
            P(),
            P(SP, None, None),
            P(SP, None, None),
            P(SP, None, None),
            P(DP, SP, None),
            P(DP, SP, None),
        ),
        out_specs=P(DP, SP, None),
        check_vma=False,
    )
```

```python
import functools

import jax
import jax.numpy as jnp
from jax import lax
from jax.experimental import pallas as pl
from jax.experimental.pallas import tpu as pltpu
from jax.sharding import Mesh
from jax.sharding import PartitionSpec as P

CH = 64
BLK = 64
GL = 256
SP = ("sp_0", "sp_1")
DP = ("x", "c")
PACK = 80
F32 = jnp.float32
BF = jnp.bfloat16


def dot(a, b, dims=((1,), (0,))):
    return lax.dot_general(a, b, (dims, ((), ())), preferred_element_type=F32)


def split3(v):
    hi = v.astype(BF)
    rest = v - hi.astype(F32)
    mid = rest.astype(BF)
    low = (rest - mid.astype(F32)).astype(BF)
    return hi, mid, low


def split2(v):
    hi = v.astype(BF)
    return hi, (v - hi.astype(F32)).astype(BF)


def tri(n):
    return (
        lax.broadcasted_iota(jnp.int32, (n, n), 0) >= lax.broadcasted_iota(jnp.int32, (n, n), 1)
    )


def same_head(rows, lanes):
    return (
        lax.broadcasted_iota(jnp.int32, (rows, lanes), 0) // CH
        == lax.broadcasted_iota(jnp.int32, (rows, lanes), 1) // CH
    )


def silu(v):
    return v / (1.0 + jnp.exp(-v))


def keys_and_logs(f_ref, floor_ref, spike_ref, group):
    f = f_ref[...].astype(F32)
    keys = (1.0 - floor_ref[...]) / (1.0 + jnp.exp(f))
    poly = jnp.full_like(keys, 1.0 / 10.0)
    for n in range(9, 0, -1):
        poly = poly * keys + 1.0 / n
    heads = spike_ref.shape[0]
    spread = (
        lax.broadcasted_iota(jnp.int32, (heads, GL), 0)
        == group * (GL // CH) + lax.broadcasted_iota(jnp.int32, (heads, GL), 1) // CH
    ).astype(BF)
    hi, mid, low = split3(spike_ref[...])
    over = ((0,), (0,))
    burst = dot(hi, spread, over) + dot(mid, spread, over) + dot(low, spread, over)
    return keys, burst - keys * poly


def running_sum(logs, length):
    lower = tri(length).astype(BF)
    out = []
    for b in range(logs.shape[0] // length):
        hi, mid, low = split3(logs[b * length : (b + 1) * length])
        out.append(dot(lower, hi) + dot(lower, mid) + dot(lower, low))
    return out


def states_kernel(f_ref, v_ref, floor_ref, spike_ref, pack_ref):
    group = pl.program_id(0)
    keys, logs = keys_and_logs(f_ref, floor_ref, spike_ref, group)
    parts = running_sum(logs, 128)
    after = jnp.zeros((1, GL), F32)
    acc = jnp.zeros((GL, GL), F32)
    for b in reversed(range(len(parts))):
        close = parts[b][127:128]
        kc = (keys[b * 128 : (b + 1) * 128] * jnp.exp(after + close - parts[b])).astype(BF)
        acc = acc + dot(v_ref[b * 128 : (b + 1) * 128, :], kc, ((0,), (0,)))
        after = after + close
    acc = jnp.where(same_head(GL, GL), acc, 0.0)
    compact = acc[0:64] + acc[64:128] + acc[128:192] + acc[192:256]
    pack_ref[0:64, :] = compact.astype(BF)
    hi, mid, low = split3(after)
    row = lax.broadcasted_iota(jnp.int32, (16, GL), 0)
    tail = jnp.where(row == 0, hi.astype(F32), 0.0)
    tail = jnp.where(row == 1, mid.astype(F32), tail)
    tail = jnp.where(row == 2, low.astype(F32), tail)
    pack_ref[64:80, :] = tail.astype(BF)


def inside_kernel(q_ref, f_ref, v_ref, floor_ref, spike_ref, out_ref, qrun_ref):
    group = pl.program_id(0)
    keys, logs = keys_and_logs(f_ref, floor_ref, spike_ref, group)
    parts = running_sum(logs, BLK)
    q = silu(q_ref[...].astype(F32))
    head_mask = same_head(GL, GL)
    lane = lax.broadcasted_iota(jnp.int32, (BLK, GL), 1)
    causal = (lane % CH) <= lax.broadcasted_iota(jnp.int32, (BLK, GL), 0)
    before = jnp.zeros((1, GL), F32)
    state = jnp.zeros((GL, GL), F32)
    zero = jnp.zeros((GL, GL), BF)
    for b in range(len(parts)):
        rows = slice(b * BLK, (b + 1) * BLK)
        cum = parts[b]
        close = cum[BLK - 1 : BLK]
        k = keys[rows]
        grow = jnp.exp(-cum)
        qd = q[rows] * jnp.exp(cum)
        qrun_ref[rows, :] = (qd * jnp.exp(before)).astype(BF)
        qd = qd.astype(BF)
        kg = (k * grow).astype(BF)
        v = v_ref[rows, :]
        k4 = jnp.where(head_mask, jnp.concatenate([kg] * 4, axis=0), zero)
        v4 = jnp.where(head_mask, jnp.concatenate([v] * 4, axis=0), zero)
        scores = dot(qd, k4, ((1,), (1,)))
        scores = jnp.where(causal, scores, 0.0).astype(BF)
        out = dot(scores, v4)
        if b > 0:
            out = out + dot(qd, state.astype(BF), ((1,), (1,)))
        out_ref[rows, :] = out
        if b + 1 < len(parts):
            kc = (k * jnp.exp(close - cum)).astype(BF)
            add = jnp.where(head_mask, dot(v, kc, ((0,), (0,))), 0.0)
            state = jnp.exp(close) * state + add
        before = before + close


def total_of(pack_ref):
    return (
        pack_ref[64:65, :].astype(F32)
        + pack_ref[65:66, :].astype(F32)
        + pack_ref[66:67, :].astype(F32)
    )


def row_kernel(pos_ref, own_ref, one_ref, two_ref, three_ref, row_ref, before_ref, btot_ref):
    here = pos_ref[0]
    width = own_ref.shape[1]
    state = jnp.zeros((CH, width), F32)
    total = jnp.zeros((1, width), F32)
    pieces = ((3, three_ref), (2, two_ref), (1, one_ref))
    for n, ref in pieces:
        use = n <= here
        t = jnp.where(use, total_of(ref), 0.0)
        state = jnp.exp(t) * state + jnp.where(use, ref[0:64, :].astype(F32), 0.0)
        total = total + t
    before_ref[...] = state
    btot_ref[...] = jnp.broadcast_to(total, (8, width))
    t = total_of(own_ref)
    state = jnp.exp(t) * state + own_ref[0:64, :].astype(F32)
    total = total + t
    for n, ref in pieces:
        use = n > here
        t = jnp.where(use, total_of(ref), 0.0)
        state = jnp.exp(t) * state + jnp.where(use, ref[0:64, :].astype(F32), 0.0)
        total = total + t
    row_ref[0:64, :] = state.astype(BF)
    hi, mid, low = split3(total)
    row = lax.broadcasted_iota(jnp.int32, (16, width), 0)
    tail = jnp.where(row == 0, hi.astype(F32), 0.0)
    tail = jnp.where(row == 1, mid.astype(F32), tail)
    tail = jnp.where(row == 2, low.astype(F32), tail)
    row_ref[64:80, :] = tail.astype(BF)


def mix_kernel(
    tok_steps,
    cap,
    pos_ref,
    out_ref,
    qrun_ref,
    gate_ref,
    res_ref,
    before_ref,
    btot_ref,
    one_ref,
    two_ref,
    three_ref,
    *refs,
):
    wmine = refs[0:4]
    wother = refs[4:8]
    scale_ref, routes_ref, upd_ref, send_ref, w_s, state_s, norm_s, pos_s = refs[8:]

    step = pl.program_id(0)
    width = gate_ref.shape[1]
    groups = width // GL
    tok_rows = routes_ref.shape[1]
    rows = gate_ref.shape[0]

    @pl.when(step == 0)
    def _():
        here = pos_ref[0]
        state = jnp.zeros((CH, width), F32)
        for n, ref in ((3, three_ref), (2, two_ref), (1, one_ref)):
            use = n <= here
            t = jnp.where(use, total_of(ref), 0.0)
            state = jnp.exp(t) * state + jnp.where(use, ref[0:64, :].astype(F32), 0.0)
        state = (jnp.exp(btot_ref[0:1, :]) * state + before_ref[...]).astype(BF)
        mask = same_head(GL, GL)
        for g in range(groups):
            one = state[:, g * GL : (g + 1) * GL]
            state_s[g] = jnp.where(mask, jnp.concatenate([one] * 4, axis=0), jnp.zeros((GL, GL), BF))
        x_here = pos_ref[1]
        core = pos_ref[2]
        piece = wmine[0].shape[0]
        for n in range(4):
            src = (x_here + 4 - n) % 4
            w_s[pl.ds((2 * src + core) * piece, piece), :] = wmine[n][...]
            w_s[pl.ds((2 * src + 1 - core) * piece, piece), :] = wother[n][...]
        experts = pos_s.shape[0]
        e = lax.broadcasted_iota(jnp.int32, (experts, tok_rows), 0)
        member = (e == routes_ref[0:1, :]) | (e == routes_ref[1:2, :])
        mem = jnp.where(member, 1.0, 0.0)
        strict = (
            lax.broadcasted_iota(jnp.int32, (tok_rows, tok_rows), 0)
            < lax.broadcasted_iota(jnp.int32, (tok_rows, tok_rows), 1)
        ).astype(BF)
        place = dot(mem.astype(BF), strict)
        pos_s[...] = jnp.where(member, place.astype(jnp.int32), -1)

    @pl.when(step < tok_steps)
    def _():
        ones = jnp.where(same_head(GL, GL), 1.0, 0.0).astype(BF)
        mixed = []
        for g in range(groups):
            lanes = slice(g * GL, (g + 1) * GL)
            o = out_ref[:, lanes] + dot(qrun_ref[:, lanes], state_s[g], ((1,), (1,)))
            hi, low = split2(o * o)
            mean = (dot(hi, ones) + dot(low, ones)) * (1.0 / CH)
            gate = silu(gate_ref[:, lanes].astype(F32))
            mixed.append((o * lax.rsqrt(mean + 1e-06) * gate).astype(BF))
        mixed = jnp.concatenate(mixed, axis=1)
        upd = (res_ref[...].astype(F32) + dot(mixed, w_s[...])).astype(BF)
        upd_ref[...] = upd
        wide = upd.astype(F32)
        mean = jnp.mean(wide * wide, axis=-1, keepdims=True)
        norm = (wide * lax.rsqrt(mean + 1e-06) * scale_ref[...]).astype(BF)
        norm_s[pl.ds(step * rows, rows), :] = norm

    @pl.when(step >= tok_steps)
    def _():
        per = send_ref.shape[0] // cap
        picks = []
        for i in range(per):
            place = pos_s[pl.ds((step - tok_steps) * per + i, 1), :]
            c = lax.broadcasted_iota(jnp.int32, (cap, tok_rows), 0)
            picks.append(jnp.where(c == place, 1.0, 0.0).astype(BF))
        send_ref[...] = dot(jnp.concatenate(picks, axis=0), norm_s[...]).astype(BF)


def serve_kernel(hid_steps, x_ref, wg_ref, wu_ref, wd_ref, out_ref, hid_s):
    step = pl.program_id(1)
    blk = wg_ref.shape[2]

    for n in range(hid_steps):

        @pl.when(step == n)
        def _(n=n):
            x = x_ref[...].reshape(hid_s.shape[0], x_ref.shape[2])
            hidden = silu(dot(x, wg_ref[0])) * dot(x, wu_ref[0])
            hid_s[:, n * blk : (n + 1) * blk] = hidden.astype(BF)

    @pl.when(step >= hid_steps)
    def _():
        out_ref[...] = dot(hid_s[...], wd_ref[0]).astype(BF).reshape(out_ref.shape)


def weights_kernel(main, routes_ref, wt_ref, main_ref, rest_ref):
    tok_rows = routes_ref.shape[1]
    experts = main_ref.shape[1] // main
    routes = jnp.transpose(routes_ref[...])
    wts = jnp.transpose(wt_ref[...])
    lane = lax.broadcasted_iota(jnp.int32, (tok_rows, 128), 1)
    strict = (
        lax.broadcasted_iota(jnp.int32, (tok_rows, tok_rows), 0)
        > lax.broadcasted_iota(jnp.int32, (tok_rows, tok_rows), 1)
    ).astype(BF)
    ones = [lane == routes[:, k : k + 1] for k in range(2)]
    place = dot(strict, jnp.where(ones[0] | ones[1], 1.0, 0.0).astype(BF))
    for ref, base in ((main_ref, 0), (rest_ref, main)):
        size = ref.shape[1] // experts
        j = lax.broadcasted_iota(jnp.int32, ref.shape, 1)
        weight = jnp.zeros(ref.shape, F32)
        for k in range(2):
            p = jnp.sum(jnp.where(ones[k], place, 0.0), axis=1, keepdims=True).astype(jnp.int32)
            p = p - base
            slot = jnp.where((p >= 0) & (p < size), routes[:, k : k + 1] * size + p, -1)
            weight = jnp.where(j == slot, wts[:, k : k + 1], weight)
        ref[...] = weight.astype(BF)


def combine_kernel(main_ref, rest_ref, got_ref, got_rest_ref, upd_ref, out_ref):
    total = dot(main_ref[...], got_ref[...]) + dot(rest_ref[...], got_rest_ref[...])
    out_ref[...] = (upd_ref[...].astype(F32) + total).astype(out_ref.dtype)


def cost(us):
    return pl.CostEstimate(flops=int(us * 5e8), bytes_accessed=int(us * 1e6), transcendentals=0)


def ring(n, size=4):
    return [(i, (i + n) % size) for i in range(size)]


def per_device(
    query_weight,
    forget_preactivation,
    written_input,
    output_gate_logit,
    forget_floor,
    extra_log_decay,
    residual,
    output_weight,
    norm_scale_vector,
    expert_gate_weight,
    expert_up_weight,
    expert_down_weight,
    routes,
    routing_weight,
):
    _, tok, width = query_weight.shape
    model = output_weight.shape[1]
    heads = width // CH
    groups = width // GL
    experts = lax.axis_size(SP)
    cap = 4 * tok // experts
    main = cap * 5 // 6
    rest = cap - main
    z = lax.axis_index("sp_0")
    y = lax.axis_index("sp_1")
    x = lax.axis_index("x")
    core = lax.axis_index("c")

    spikes = lax.dynamic_slice_in_dim(extra_log_decay[0].T, lax.axis_index(SP) * tok, tok, 1)
    q, f, v, gate = (
        a.reshape(tok, width)
        for a in (query_weight, forget_preactivation, written_input, output_gate_logit)
    )
    floor = forget_floor.reshape(1, width)
    scale = norm_scale_vector.reshape(1, model)
    res = residual.reshape(tok, model)

    mine = output_weight
    wmine = [lax.ppermute(mine, "x", ring(n)) for n in (1, 2, 3)]

    tall = pl.BlockSpec((tok, GL), lambda g: (0, g))
    flat = pl.BlockSpec((1, GL), lambda g: (0, g))
    whole = pl.BlockSpec((heads, tok), lambda g: (0, 0))
    pack = pl.pallas_call(
        states_kernel,
        grid=(groups,),
        in_specs=[tall, tall, flat, whole],
        out_specs=pl.BlockSpec((PACK, GL), lambda g: (0, g)),
        out_shape=jax.ShapeDtypeStruct((PACK, width), BF),
        cost_estimate=cost(7),
        name="states",
    )(f, v, floor, spikes)

    along_y = [lax.ppermute(pack, "sp_1", ring(n)) for n in (1, 2, 3)]


    vm = pl.BlockSpec(memory_space=pltpu.VMEM)
    sm = pl.BlockSpec(memory_space=pltpu.SMEM)
    row, before, btot = pl.pallas_call(
        row_kernel,
        in_specs=[sm, vm, vm, vm, vm],
        out_specs=[vm, vm, vm],
        out_shape=[
            jax.ShapeDtypeStruct((PACK, width), BF),
            jax.ShapeDtypeStruct((CH, width), F32),
            jax.ShapeDtypeStruct((8, width), F32),
        ],
        cost_estimate=cost(2),
        name="row",
    )(y.astype(jnp.int32).reshape(1), pack, *along_y)

    along_z = [lax.ppermute(row, "sp_0", ring(n)) for n in (1, 2, 3)]

    q, row = lax.optimization_barrier((q, row))
    inside, qrun = pl.pallas_call(
        inside_kernel,
        grid=(groups,),
        in_specs=[tall, tall, tall, flat, whole],
        out_specs=[tall, tall],
        out_shape=[jax.ShapeDtypeStruct((tok, width), F32), jax.ShapeDtypeStruct((tok, width), BF)],
        cost_estimate=cost(8),
        name="inside",
    )(q, f, v, floor, spikes)

    wmine, qrun = lax.optimization_barrier((wmine, qrun))
    wmine = [mine] + wmine
    wother = [lax.ppermute(p, "c", ring(1, 2)) for p in wmine]


    route_rows = jnp.pad(routes[0].T, ((0, 6), (0, 0)), constant_values=-1)
    place = jnp.stack([z, x, core]).astype(jnp.int32)
    tok_steps = 3
    rows = tok // tok_steps
    send_steps = 4
    send_rows = experts * cap // send_steps
    clip = lambda i: jnp.minimum(i, tok_steps - 1)
    tok_w = pl.BlockSpec((rows, width), lambda i: (clip(i), 0))
    tok_m = pl.BlockSpec((rows, model), lambda i: (clip(i), 0))
    full = lambda a: pl.BlockSpec(a.shape, lambda i: (0,) * a.ndim)


    updated, send = pl.pallas_call(
        functools.partial(mix_kernel, tok_steps, cap),
        grid=(tok_steps + send_steps,),
        in_specs=[
            sm,
            tok_w,
            tok_w,
            tok_w,
            tok_m,
            full(before),
            full(btot),
            full(row),
            full(row),
            full(row),
            *[full(mine)] * 8,
            full(scale),
            full(route_rows),
        ],
        out_specs=[
            tok_m,
            pl.BlockSpec((send_rows, model), lambda i: (jnp.maximum(i - tok_steps, 0), 0)),
        ],
        out_shape=[
            jax.ShapeDtypeStruct((tok, model), BF),
            jax.ShapeDtypeStruct((experts * cap, model), BF),
        ],
        scratch_shapes=[
            pltpu.VMEM((width, model), BF),
            pltpu.VMEM((groups, GL, GL), BF),
            pltpu.VMEM((tok, model), BF),
            pltpu.VMEM((experts, tok), jnp.int32),
        ],
        compiler_params=pltpu.CompilerParams(vmem_limit_bytes=50 * 1024 * 1024),
        cost_estimate=cost(12),
        name="mix",
    )(place, inside, qrun, gate, res, before, btot, *along_z, *wmine, *wother, scale, route_rows)

    def exchange(a):
        return lax.all_to_all(a, SP, split_axis=0, concat_axis=0, tiled=True)

    hid = expert_gate_weight.shape[2]
    hid_steps = 2
    out_steps = 2

    def serve(arrived, first, size, blocks):
        srcs = experts // blocks
        where = first // size
        up = pl.BlockSpec(
            (1, model, hid // hid_steps), lambda m, j: (0, 0, jnp.minimum(j, hid_steps - 1))
        )
        after = lambda j: jnp.maximum(j - hid_steps, 0)
        return pl.pallas_call(
            functools.partial(serve_kernel, hid_steps),
            grid=(blocks, hid_steps + out_steps),
            in_specs=[
                pl.BlockSpec((srcs, size, model), lambda m, j: (m, where, 0)),
                up,
                up,
                pl.BlockSpec((1, hid, model // out_steps), lambda m, j: (0, 0, after(j))),
            ],
            out_specs=pl.BlockSpec((srcs, size, model // out_steps), lambda m, j: (m, 0, after(j))),
            out_shape=jax.ShapeDtypeStruct((experts, size, model), BF),
            scratch_shapes=[pltpu.VMEM((srcs * size, hid), BF)],
            compiler_params=pltpu.CompilerParams(vmem_limit_bytes=50 * 1024 * 1024),
            cost_estimate=cost(18 if blocks > 1 else 5),
            name="serve",
        )(arrived, expert_gate_weight, expert_up_weight, expert_down_weight)

    arrived = exchange(send.reshape(experts, cap, model))
    served_rest = serve(arrived, main, rest, 1)
    got_rest = exchange(served_rest)

    picks, _ = lax.optimization_barrier((route_rows, served_rest))
    weights_main, weights_rest = pl.pallas_call(
        functools.partial(weights_kernel, main),
        in_specs=[vm, vm],
        out_specs=[vm, vm],
        out_shape=[
            jax.ShapeDtypeStruct((tok, experts * main), BF),
            jax.ShapeDtypeStruct((tok, experts * rest), BF),
        ],
        cost_estimate=cost(2),
        name="weights",
    )(picks, jnp.pad(routing_weight[0].T, ((0, 6), (0, 0))))
    arrived, weights_main, weights_rest = lax.optimization_barrier(
        (arrived, weights_main, weights_rest)
    )
    got = exchange(serve(arrived, 0, main, 2))

    blk = 512
    col = lambda r: pl.BlockSpec((r, blk), lambda i: (0, i))
    layer_out = pl.pallas_call(
        combine_kernel,
        grid=(model // blk,),
        in_specs=[
            full(weights_main),
            full(weights_rest),
            col(experts * main),
            col(experts * rest),
            col(tok),
        ],
        out_specs=col(tok),
        out_shape=jax.ShapeDtypeStruct((tok, model), BF),
        cost_estimate=cost(4),
        name="combine",
    )(
        weights_main,
        weights_rest,
        got.reshape(experts * main, model),
        got_rest.reshape(experts * rest, model),
        updated,
    )
    return layer_out.reshape(1, tok, model)


def solution(mesh):
    torus = Mesh(
        mesh.devices.reshape(4, 4, 4, mesh.shape["dp"] // 4), ("sp_0", "sp_1", "x", "c")
    )
    return jax.shard_map(
        per_device,
        mesh=torus,
        in_specs=(
            P(DP, SP, None),
            P(DP, SP, None),
            P(DP, SP, None),
            P(DP, SP, None),
            P(),
            P(DP, None, None),
            P(DP, SP, None),
            P(DP, None),
            P(),
            P(SP, None, None),
            P(SP, None, None),
            P(SP, None, None),
            P(DP, SP, None),
            P(DP, SP, None),
        ),
        out_specs=P(DP, SP, None),
        check_vma=False,
    )
```

```python
import functools

import jax
import jax.numpy as jnp
from jax import lax
from jax.experimental import pallas as pl
from jax.experimental.pallas import tpu as pltpu
from jax.sharding import Mesh
from jax.sharding import PartitionSpec as P

CH = 64
BLK = 64
GL = 256
SP = ("sp_0", "sp_1")
DP = ("x", "c")
PACK = 80
F32 = jnp.float32
BF = jnp.bfloat16


def dot(a, b, dims=((1,), (0,))):
    return lax.dot_general(a, b, (dims, ((), ())), preferred_element_type=F32)


def split3(v):
    hi = v.astype(BF)
    rest = v - hi.astype(F32)
    mid = rest.astype(BF)
    low = (rest - mid.astype(F32)).astype(BF)
    return hi, mid, low


def split2(v):
    hi = v.astype(BF)
    return hi, (v - hi.astype(F32)).astype(BF)


def tri(n):
    return (
        lax.broadcasted_iota(jnp.int32, (n, n), 0) >= lax.broadcasted_iota(jnp.int32, (n, n), 1)
    )


def same_head(rows, lanes):
    return (
        lax.broadcasted_iota(jnp.int32, (rows, lanes), 0) // CH
        == lax.broadcasted_iota(jnp.int32, (rows, lanes), 1) // CH
    )


def silu(v):
    return v / (1.0 + jnp.exp(-v))


def keys_and_logs(f_ref, floor_ref, spike_ref, group):
    f = f_ref[...].astype(F32)
    keys = (1.0 - floor_ref[...]) / (1.0 + jnp.exp(f))
    poly = jnp.full_like(keys, 1.0 / 10.0)
    for n in range(9, 0, -1):
        poly = poly * keys + 1.0 / n
    heads = spike_ref.shape[0]
    spread = (
        lax.broadcasted_iota(jnp.int32, (heads, GL), 0)
        == group * (GL // CH) + lax.broadcasted_iota(jnp.int32, (heads, GL), 1) // CH
    ).astype(BF)
    hi, mid, low = split3(spike_ref[...])
    over = ((0,), (0,))
    burst = dot(hi, spread, over) + dot(mid, spread, over) + dot(low, spread, over)
    return keys, burst - keys * poly


def running_sum(logs, length):
    lower = tri(length).astype(BF)
    out = []
    for b in range(logs.shape[0] // length):
        hi, mid, low = split3(logs[b * length : (b + 1) * length])
        out.append(dot(lower, hi) + dot(lower, mid) + dot(lower, low))
    return out


def states_kernel(f_ref, v_ref, floor_ref, spike_ref, pack_ref):
    group = pl.program_id(0)
    keys, logs = keys_and_logs(f_ref, floor_ref, spike_ref, group)
    parts = running_sum(logs, 128)
    after = jnp.zeros((1, GL), F32)
    acc = jnp.zeros((GL, GL), F32)
    for b in reversed(range(len(parts))):
        close = parts[b][127:128]
        kc = (keys[b * 128 : (b + 1) * 128] * jnp.exp(after + close - parts[b])).astype(BF)
        acc = acc + dot(v_ref[b * 128 : (b + 1) * 128, :], kc, ((0,), (0,)))
        after = after + close
    acc = jnp.where(same_head(GL, GL), acc, 0.0)
    compact = acc[0:64] + acc[64:128] + acc[128:192] + acc[192:256]
    pack_ref[0:64, :] = compact.astype(BF)
    hi, mid, low = split3(after)
    row = lax.broadcasted_iota(jnp.int32, (16, GL), 0)
    tail = jnp.where(row == 0, hi.astype(F32), 0.0)
    tail = jnp.where(row == 1, mid.astype(F32), tail)
    tail = jnp.where(row == 2, low.astype(F32), tail)
    pack_ref[64:80, :] = tail.astype(BF)


def inside_kernel(q_ref, f_ref, v_ref, floor_ref, spike_ref, out_ref, qrun_ref):
    group = pl.program_id(0)
    keys, logs = keys_and_logs(f_ref, floor_ref, spike_ref, group)
    parts = running_sum(logs, BLK)
    q = silu(q_ref[...].astype(F32))
    head_mask = same_head(GL, GL)
    lane = lax.broadcasted_iota(jnp.int32, (BLK, GL), 1)
    causal = (lane % CH) <= lax.broadcasted_iota(jnp.int32, (BLK, GL), 0)
    before = jnp.zeros((1, GL), F32)
    state = jnp.zeros((GL, GL), F32)
    zero = jnp.zeros((GL, GL), BF)
    for b in range(len(parts)):
        rows = slice(b * BLK, (b + 1) * BLK)
        cum = parts[b]
        close = cum[BLK - 1 : BLK]
        k = keys[rows]
        grow = jnp.exp(-cum)
        qd = q[rows] * jnp.exp(cum)
        qrun_ref[rows, :] = (qd * jnp.exp(before)).astype(BF)
        qd = qd.astype(BF)
        kg = (k * grow).astype(BF)
        v = v_ref[rows, :]
        k4 = jnp.where(head_mask, jnp.concatenate([kg] * 4, axis=0), zero)
        v4 = jnp.where(head_mask, jnp.concatenate([v] * 4, axis=0), zero)
        scores = dot(qd, k4, ((1,), (1,)))
        scores = jnp.where(causal, scores, 0.0).astype(BF)
        out = dot(scores, v4)
        if b > 0:
            out = out + dot(qd, state.astype(BF), ((1,), (1,)))
        out_ref[rows, :] = out
        if b + 1 < len(parts):
            kc = (k * jnp.exp(close - cum)).astype(BF)
            add = jnp.where(head_mask, dot(v, kc, ((0,), (0,))), 0.0)
            state = jnp.exp(close) * state + add
        before = before + close


def total_of(pack_ref):
    return (
        pack_ref[64:65, :].astype(F32)
        + pack_ref[65:66, :].astype(F32)
        + pack_ref[66:67, :].astype(F32)
    )


def row_kernel(pos_ref, own_ref, one_ref, two_ref, three_ref, row_ref, before_ref, btot_ref):
    here = pos_ref[0]
    width = own_ref.shape[1]
    state = jnp.zeros((CH, width), F32)
    total = jnp.zeros((1, width), F32)
    pieces = ((3, three_ref), (2, two_ref), (1, one_ref))
    for n, ref in pieces:
        use = n <= here
        t = jnp.where(use, total_of(ref), 0.0)
        state = jnp.exp(t) * state + jnp.where(use, ref[0:64, :].astype(F32), 0.0)
        total = total + t
    before_ref[...] = state
    btot_ref[...] = jnp.broadcast_to(total, (8, width))
    t = total_of(own_ref)
    state = jnp.exp(t) * state + own_ref[0:64, :].astype(F32)
    total = total + t
    for n, ref in pieces:
        use = n > here
        t = jnp.where(use, total_of(ref), 0.0)
        state = jnp.exp(t) * state + jnp.where(use, ref[0:64, :].astype(F32), 0.0)
        total = total + t
    row_ref[0:64, :] = state.astype(BF)
    hi, mid, low = split3(total)
    row = lax.broadcasted_iota(jnp.int32, (16, width), 0)
    tail = jnp.where(row == 0, hi.astype(F32), 0.0)
    tail = jnp.where(row == 1, mid.astype(F32), tail)
    tail = jnp.where(row == 2, low.astype(F32), tail)
    row_ref[64:80, :] = tail.astype(BF)


def mix_kernel(
    tok_steps,
    cap,
    pos_ref,
    out_ref,
    qrun_ref,
    gate_ref,
    res_ref,
    before_ref,
    btot_ref,
    one_ref,
    two_ref,
    three_ref,
    *refs,
):
    wmine = refs[0:4]
    wother = refs[4:8]
    scale_ref, routes_ref, upd_ref, send_ref, w_s, state_s, norm_s, pos_s, sems = refs[8:]

    step = pl.program_id(0)
    width = gate_ref.shape[1]
    groups = width // GL
    tok_rows = routes_ref.shape[1]
    rows = gate_ref.shape[0]

    piece = wmine[0].shape[0]

    def weight_copies():
        for n in range(4):
            src = (pos_ref[1] + 4 - n) % 4
            for i, (ref, core) in enumerate(((wmine[n], pos_ref[2]), (wother[n], 1 - pos_ref[2]))):
                where = pl.ds(pl.multiple_of((2 * src + core) * piece, piece), piece)
                yield pltpu.make_async_copy(ref, w_s.at[where], sems.at[2 * n + i])

    @pl.when(step == 0)
    def _():
        for c in weight_copies():
            c.start()
        here = pos_ref[0]
        state = jnp.zeros((CH, width), F32)
        for n, ref in ((3, three_ref), (2, two_ref), (1, one_ref)):
            use = n <= here
            t = jnp.where(use, total_of(ref), 0.0)
            state = jnp.exp(t) * state + jnp.where(use, ref[0:64, :].astype(F32), 0.0)
        state = (jnp.exp(btot_ref[0:1, :]) * state + before_ref[...]).astype(BF)
        mask = same_head(GL, GL)
        for g in range(groups):
            one = state[:, g * GL : (g + 1) * GL]
            state_s[g] = jnp.where(mask, jnp.concatenate([one] * 4, axis=0), jnp.zeros((GL, GL), BF))
        experts = pos_s.shape[0]
        e = lax.broadcasted_iota(jnp.int32, (experts, tok_rows), 0)
        member = (e == routes_ref[0:1, :]) | (e == routes_ref[1:2, :])
        mem = jnp.where(member, 1.0, 0.0)
        strict = (
            lax.broadcasted_iota(jnp.int32, (tok_rows, tok_rows), 0)
            < lax.broadcasted_iota(jnp.int32, (tok_rows, tok_rows), 1)
        ).astype(BF)
        place = dot(mem.astype(BF), strict)
        pos_s[...] = jnp.where(member, place.astype(jnp.int32), -1)

    @pl.when(step < tok_steps)
    def _():
        ones = jnp.where(same_head(GL, GL), 1.0, 0.0).astype(BF)
        mixed = []
        for g in range(groups):
            lanes = slice(g * GL, (g + 1) * GL)
            o = out_ref[:, lanes] + dot(qrun_ref[:, lanes], state_s[g], ((1,), (1,)))
            hi, low = split2(o * o)
            mean = (dot(hi, ones) + dot(low, ones)) * (1.0 / CH)
            gate = silu(gate_ref[:, lanes].astype(F32))
            mixed.append((o * lax.rsqrt(mean + 1e-06) * gate).astype(BF))
        mixed = jnp.concatenate(mixed, axis=1)

        @pl.when(step == 0)
        def _():
            for c in weight_copies():
                c.wait()

        upd = (res_ref[...].astype(F32) + dot(mixed, w_s[...])).astype(BF)
        upd_ref[...] = upd
        wide = upd.astype(F32)
        mean = jnp.mean(wide * wide, axis=-1, keepdims=True)
        norm = (wide * lax.rsqrt(mean + 1e-06) * scale_ref[...]).astype(BF)
        norm_s[pl.ds(step * rows, rows), :] = norm

    @pl.when(step >= tok_steps)
    def _():
        per = send_ref.shape[0] // cap
        picks = []
        for i in range(per):
            place = pos_s[pl.ds((step - tok_steps) * per + i, 1), :]
            c = lax.broadcasted_iota(jnp.int32, (cap, tok_rows), 0)
            picks.append(jnp.where(c == place, 1.0, 0.0).astype(BF))
        send_ref[...] = dot(jnp.concatenate(picks, axis=0), norm_s[...]).astype(BF)


def serve_kernel(
    first, parts, x_ref, wg_ref, wu_ref, wd_ref, out_ref, x_s, wg_s, wu_s, wd_s, hid_s, out_s, sems, out_sems
):
    srcs, size, model = x_s.shape
    hid = hid_s.shape[1]
    steps = 4
    hb = hid // steps
    ob = model // steps
    per = srcs // parts
    rows = per * size

    def x_copy(m):
        lo = m * per
        return pltpu.make_async_copy(
            x_ref.at[pl.ds(lo, per), pl.ds(first, size), :], x_s.at[pl.ds(lo, per)], sems.at[m]
        )

    def w_copy(which, n):
        src, dst, cols = ((wg_ref, wg_s, hb), (wu_ref, wu_s, hb), (wd_ref, wd_s, ob))[which]
        lanes = pl.ds(n * cols, cols)
        return pltpu.make_async_copy(
            src.at[0, :, lanes], dst.at[:, lanes], sems.at[parts + which * steps + n]
        )

    def out_copy(m, n):
        lanes = pl.ds(n * ob, ob)
        return pltpu.make_async_copy(
            out_s.at[pl.ds(m * per, per), :, lanes],
            out_ref.at[pl.ds(m * per, per), :, lanes],
            out_sems.at[m * steps + n],
        )

    x_copy(0).start()
    w_copy(0, 0).start()
    w_copy(1, 0).start()
    for m in range(1, parts):
        x_copy(m).start()
    x_copy(0).wait()
    w_copy(0, 0).wait()
    w_copy(1, 0).wait()
    for n in range(1, steps):
        w_copy(0, n).start()
        w_copy(1, n).start()
    for n in range(steps):
        w_copy(2, n).start()
    for n in range(steps):
        lanes = slice(n * hb, (n + 1) * hb)
        if n > 0:
            w_copy(0, n).wait()
            w_copy(1, n).wait()
        for m in range(parts):
            if n == 0 and m > 0:
                x_copy(m).wait()
            x = x_s[m * per : (m + 1) * per].reshape(rows, model)
            hidden = silu(dot(x, wg_s[:, lanes])) * dot(x, wu_s[:, lanes])
            hid_s[m * rows : (m + 1) * rows, lanes] = hidden.astype(BF)
    for n in range(steps):
        lanes = slice(n * ob, (n + 1) * ob)
        w_copy(2, n).wait()
        for m in range(parts):
            got = dot(hid_s[m * rows : (m + 1) * rows, :], wd_s[:, lanes]).astype(BF)
            out_s[m * per : (m + 1) * per, :, lanes] = got.reshape(per, size, ob)
            out_copy(m, n).start()
    for n in range(steps):
        for m in range(parts):
            out_copy(m, n).wait()


def serve_rest_kernel(
    first, parts, x_ref, wg_ref, wu_ref, wd_ref, out_ref, x_s, wd_s, hid_s, out_s, sems, wd_sems, out_sems
):
    srcs, size, model = x_s.shape
    hid = hid_s.shape[1]
    steps = 4
    hb = hid // steps
    ob = model // steps
    per = srcs // parts
    rows = per * size

    def x_copy(m):
        lo = m * per
        return pltpu.make_async_copy(
            x_ref.at[pl.ds(lo, per), pl.ds(first, size), :], x_s.at[pl.ds(lo, per)], sems.at[m]
        )

    def wd_copy(n):
        lanes = pl.ds(n * ob, ob)
        return pltpu.make_async_copy(wd_ref.at[0, :, lanes], wd_s.at[:, lanes], wd_sems.at[n])

    def out_copy(m, n):
        lanes = pl.ds(n * ob, ob)
        return pltpu.make_async_copy(
            out_s.at[pl.ds(m * per, per), :, lanes],
            out_ref.at[pl.ds(m * per, per), :, lanes],
            out_sems.at[m * steps + n],
        )

    for m in range(parts):
        x_copy(m).start()
    for n in range(steps):
        wd_copy(n).start()
    for n in range(steps):
        lanes = slice(n * hb, (n + 1) * hb)
        for m in range(parts):
            if n == 0:
                x_copy(m).wait()
            x = x_s[m * per : (m + 1) * per].reshape(rows, model)
            hidden = silu(dot(x, wg_ref[0, :, lanes])) * dot(x, wu_ref[0, :, lanes])
            hid_s[m * rows : (m + 1) * rows, lanes] = hidden.astype(BF)
    for n in range(steps):
        lanes = slice(n * ob, (n + 1) * ob)
        wd_copy(n).wait()
        for m in range(parts):
            got = dot(hid_s[m * rows : (m + 1) * rows, :], wd_s[:, lanes]).astype(BF)
            out_s[m * per : (m + 1) * per, :, lanes] = got.reshape(per, size, ob)
            out_copy(m, n).start()
    for n in range(steps):
        for m in range(parts):
            out_copy(m, n).wait()


def weights_kernel(main, routes_ref, wt_ref, main_ref, rest_ref):
    tok_rows = routes_ref.shape[1]
    experts = main_ref.shape[1] // main
    routes = jnp.transpose(routes_ref[...])
    wts = jnp.transpose(wt_ref[...])
    lane = lax.broadcasted_iota(jnp.int32, (tok_rows, 128), 1)
    strict = (
        lax.broadcasted_iota(jnp.int32, (tok_rows, tok_rows), 0)
        > lax.broadcasted_iota(jnp.int32, (tok_rows, tok_rows), 1)
    ).astype(BF)
    ones = [lane == routes[:, k : k + 1] for k in range(2)]
    place = dot(strict, jnp.where(ones[0] | ones[1], 1.0, 0.0).astype(BF))
    for ref, base in ((main_ref, 0), (rest_ref, main)):
        size = ref.shape[1] // experts
        j = lax.broadcasted_iota(jnp.int32, ref.shape, 1)
        weight = jnp.zeros(ref.shape, F32)
        for k in range(2):
            p = jnp.sum(jnp.where(ones[k], place, 0.0), axis=1, keepdims=True).astype(jnp.int32)
            p = p - base
            slot = jnp.where((p >= 0) & (p < size), routes[:, k : k + 1] * size + p, -1)
            weight = jnp.where(j == slot, wts[:, k : k + 1], weight)
        ref[...] = weight.astype(BF)


def combine_kernel(main_ref, rest_ref, got_ref, got_rest_ref, upd_ref, out_ref, out_s, sems):
    steps = sems.shape[0]
    blk = out_s.shape[1] // steps

    def out_copy(n):
        lanes = pl.ds(n * blk, blk)
        return pltpu.make_async_copy(out_s.at[:, lanes], out_ref.at[:, lanes], sems.at[n])

    for n in range(steps):
        lanes = slice(n * blk, (n + 1) * blk)
        total = dot(main_ref[...], got_ref[:, lanes]) + dot(rest_ref[...], got_rest_ref[:, lanes])
        out_s[:, lanes] = (upd_ref[:, lanes].astype(F32) + total).astype(out_s.dtype)
        out_copy(n).start()
    for n in range(steps):
        out_copy(n).wait()


def cost(us):
    return pl.CostEstimate(flops=int(us * 5e8), bytes_accessed=int(us * 1e6), transcendentals=0)


def ring(n, size=4):
    return [(i, (i + n) % size) for i in range(size)]


def per_device(
    query_weight,
    forget_preactivation,
    written_input,
    output_gate_logit,
    forget_floor,
    extra_log_decay,
    residual,
    output_weight,
    norm_scale_vector,
    expert_gate_weight,
    expert_up_weight,
    expert_down_weight,
    routes,
    routing_weight,
):
    _, tok, width = query_weight.shape
    model = output_weight.shape[1]
    heads = width // CH
    groups = width // GL
    experts = lax.axis_size(SP)
    cap = 4 * tok // experts
    main = cap * 5 // 6
    rest = cap - main
    z = lax.axis_index("sp_0")
    y = lax.axis_index("sp_1")
    x = lax.axis_index("x")
    core = lax.axis_index("c")

    spikes = lax.dynamic_slice_in_dim(extra_log_decay[0].T, lax.axis_index(SP) * tok, tok, 1)
    q, f, v, gate = (
        a.reshape(tok, width)
        for a in (query_weight, forget_preactivation, written_input, output_gate_logit)
    )
    floor = forget_floor.reshape(1, width)
    scale = norm_scale_vector.reshape(1, model)
    res = residual.reshape(tok, model)

    mine = output_weight
    wmine = [lax.ppermute(mine, "x", ring(n)) for n in (1, 2, 3)]

    tall = pl.BlockSpec((tok, GL), lambda g: (0, g))
    flat = pl.BlockSpec((1, GL), lambda g: (0, g))
    whole = pl.BlockSpec((heads, tok), lambda g: (0, 0))
    pack = pl.pallas_call(
        states_kernel,
        grid=(groups,),
        in_specs=[tall, tall, flat, whole],
        out_specs=pl.BlockSpec((PACK, GL), lambda g: (0, g)),
        out_shape=jax.ShapeDtypeStruct((PACK, width), BF),
        cost_estimate=cost(7),
        compiler_params=pltpu.CompilerParams(vmem_limit_bytes=66 * 1000 * 1000),
        name="states",
    )(f, v, floor, spikes)

    along_y = [lax.ppermute(pack, "sp_1", ring(n)) for n in (1, 2, 3)]


    vm = pl.BlockSpec(memory_space=pltpu.VMEM)
    sm = pl.BlockSpec(memory_space=pltpu.SMEM)

    inside, qrun = pl.pallas_call(
        inside_kernel,
        grid=(groups,),
        in_specs=[tall, tall, tall, flat, whole],
        out_specs=[tall, tall],
        out_shape=[jax.ShapeDtypeStruct((tok, width), F32), jax.ShapeDtypeStruct((tok, width), BF)],
        cost_estimate=cost(8),
        compiler_params=pltpu.CompilerParams(vmem_limit_bytes=66 * 1000 * 1000),
        name="inside",
    )(q, f, v, floor, spikes)

    row, before, btot = pl.pallas_call(
        row_kernel,
        in_specs=[sm, vm, vm, vm, vm],
        out_specs=[vm, vm, vm],
        out_shape=[
            jax.ShapeDtypeStruct((PACK, width), BF),
            jax.ShapeDtypeStruct((CH, width), F32),
            jax.ShapeDtypeStruct((8, width), F32),
        ],
        cost_estimate=cost(2),
        compiler_params=pltpu.CompilerParams(vmem_limit_bytes=66 * 1000 * 1000),
        name="row",
    )(y.astype(jnp.int32).reshape(1), pack, *along_y)

    along_z = [lax.ppermute(row, "sp_0", ring(n)) for n in (1, 2, 3)]

    wmine, row = lax.optimization_barrier((wmine, row))
    wmine = [mine] + wmine
    wother = [lax.ppermute(p, "c", ring(1, 2)) for p in wmine]

    route_rows = jnp.pad(routes[0].T, ((0, 6), (0, 0)), constant_values=-1)
    wt_rows = jnp.pad(routing_weight[0].T, ((0, 6), (0, 0)))
    route_rows, wt_rows, row = lax.optimization_barrier((route_rows, wt_rows, row))
    weights_main, weights_rest = pl.pallas_call(
        functools.partial(weights_kernel, main),
        in_specs=[vm, vm],
        out_specs=[vm, vm],
        out_shape=[
            jax.ShapeDtypeStruct((tok, experts * main), BF),
            jax.ShapeDtypeStruct((tok, experts * rest), BF),
        ],
        cost_estimate=cost(2),
        compiler_params=pltpu.CompilerParams(vmem_limit_bytes=66 * 1000 * 1000),
        name="weights",
    )(route_rows, wt_rows)


    place = jnp.stack([z, x, core]).astype(jnp.int32)
    tok_steps = 3
    rows = tok // tok_steps
    send_steps = 4
    send_rows = experts * cap // send_steps
    clip = lambda i: jnp.minimum(i, tok_steps - 1)
    tok_w = pl.BlockSpec((rows, width), lambda i: (clip(i), 0))
    tok_m = pl.BlockSpec((rows, model), lambda i: (clip(i), 0))
    full = lambda a: pl.BlockSpec(a.shape, lambda i: (0,) * a.ndim)


    updated, send = pl.pallas_call(
        functools.partial(mix_kernel, tok_steps, cap),
        grid=(tok_steps + send_steps,),
        in_specs=[
            sm,
            tok_w,
            tok_w,
            tok_w,
            tok_m,
            full(before),
            full(btot),
            full(row),
            full(row),
            full(row),
            *[pl.BlockSpec(memory_space=pl.ANY)] * 8,
            full(scale),
            full(route_rows),
        ],
        out_specs=[
            tok_m,
            pl.BlockSpec((send_rows, model), lambda i: (jnp.maximum(i - tok_steps, 0), 0)),
        ],
        out_shape=[
            jax.ShapeDtypeStruct((tok, model), BF),
            jax.ShapeDtypeStruct((experts * cap, model), BF),
        ],
        scratch_shapes=[
            pltpu.VMEM((width, model), BF),
            pltpu.VMEM((groups, GL, GL), BF),
            pltpu.VMEM((tok, model), BF),
            pltpu.VMEM((experts, tok), jnp.int32),
            pltpu.SemaphoreType.DMA((8,)),
        ],
        compiler_params=pltpu.CompilerParams(vmem_limit_bytes=66 * 1000 * 1000),
        cost_estimate=cost(12),
        name="mix",
    )(place, inside, qrun, gate, res, before, btot, *along_z, *wmine, *wother, scale, route_rows)

    def exchange(a):
        return lax.all_to_all(a, SP, split_axis=0, concat_axis=0, tiled=True)

    hid = expert_gate_weight.shape[2]
    anywhere = pl.BlockSpec(memory_space=pl.ANY)

    dma = lambda n: pltpu.SemaphoreType.DMA((n,))

    def serve(kernel, arrived, first, size, parts, scratch, specs, limit, us):
        return pl.pallas_call(
            functools.partial(kernel, first, parts),
            in_specs=[anywhere, *specs],
            out_specs=anywhere,
            out_shape=jax.ShapeDtypeStruct((experts, size, model), BF),
            scratch_shapes=[
                pltpu.VMEM((experts, size, model), BF),
                *[pltpu.VMEM(shape, BF) for shape in scratch],
                pltpu.VMEM((experts * size, hid), BF),
                pltpu.VMEM((experts, size, model), BF),
                *([dma(parts), dma(4)] if kernel is serve_rest_kernel else [dma(parts + 12)]),
                dma(parts * 4),
            ],
            compiler_params=pltpu.CompilerParams(vmem_limit_bytes=limit * 1024 * 1024),
            cost_estimate=cost(us),
            name="serve",
        )(arrived, expert_gate_weight, expert_up_weight, expert_down_weight)

    def serve_main(arrived):
        scratch = [(model, hid), (model, hid), (hid, model)]
        return serve(serve_kernel, arrived, 0, main, 2, scratch, [anywhere] * 3, 50, 20)

    def serve_rest(arrived):
        specs = [vm, vm, anywhere]
        return serve(serve_rest_kernel, arrived, main, rest, 1, [(hid, model)], specs, 36, 5)

    arrived = exchange(send.reshape(experts, cap, model))
    served_rest = serve_rest(arrived)
    got_rest = exchange(served_rest)

    got = exchange(serve_main(arrived))

    layer_out = pl.pallas_call(
        combine_kernel,
        in_specs=[vm] * 5,
        out_specs=anywhere,
        out_shape=jax.ShapeDtypeStruct((tok, model), BF),
        scratch_shapes=[pltpu.VMEM((tok, model), BF), pltpu.SemaphoreType.DMA((4,))],
        compiler_params=pltpu.CompilerParams(vmem_limit_bytes=40 * 1024 * 1024),
        cost_estimate=cost(4),
        name="combine",
    )(
        weights_main,
        weights_rest,
        got.reshape(experts * main, model),
        got_rest.reshape(experts * rest, model),
        updated,
    )
    return layer_out.reshape(1, tok, model)


def solution(mesh):
    torus = Mesh(
        mesh.devices.reshape(4, 4, 4, mesh.shape["dp"] // 4), ("sp_0", "sp_1", "x", "c")
    )
    return jax.shard_map(
        per_device,
        mesh=torus,
        in_specs=(
            P(DP, SP, None),
            P(DP, SP, None),
            P(DP, SP, None),
            P(DP, SP, None),
            P(),
            P(DP, None, None),
            P(DP, SP, None),
            P(DP, None),
            P(),
            P(SP, None, None),
            P(SP, None, None),
            P(SP, None, None),
            P(DP, SP, None),
            P(DP, SP, None),
        ),
        out_specs=P(DP, SP, None),
        check_vma=False,
    )
```

```python
import functools

import jax
import jax.numpy as jnp
from jax import lax
from jax.experimental import pallas as pl
from jax.experimental.pallas import tpu as pltpu
from jax.sharding import Mesh
from jax.sharding import PartitionSpec as P

CH = 64
BLK = 64
GL = 256
SP = ("sp_0", "sp_1")
DP = ("x", "c")
PACK = 80
F32 = jnp.float32
BF = jnp.bfloat16


def dot(a, b, dims=((1,), (0,))):
    return lax.dot_general(a, b, (dims, ((), ())), preferred_element_type=F32)


def split3(v):
    hi = v.astype(BF)
    rest = v - hi.astype(F32)
    mid = rest.astype(BF)
    low = (rest - mid.astype(F32)).astype(BF)
    return hi, mid, low


def split2(v):
    hi = v.astype(BF)
    return hi, (v - hi.astype(F32)).astype(BF)


def tri(n):
    return (
        lax.broadcasted_iota(jnp.int32, (n, n), 0) >= lax.broadcasted_iota(jnp.int32, (n, n), 1)
    )


def same_head(rows, lanes):
    return (
        lax.broadcasted_iota(jnp.int32, (rows, lanes), 0) // CH
        == lax.broadcasted_iota(jnp.int32, (rows, lanes), 1) // CH
    )


def silu(v):
    return v / (1.0 + jnp.exp(-v))


def keys_and_logs(f_ref, floor_ref, spike_ref, group):
    f = f_ref[...].astype(F32)
    keys = (1.0 - floor_ref[...]) / (1.0 + jnp.exp(f))
    poly = jnp.full_like(keys, 1.0 / 7.0)
    for n in range(6, 0, -1):
        poly = poly * keys + 1.0 / n
    heads = spike_ref.shape[0]
    spread = (
        lax.broadcasted_iota(jnp.int32, (heads, GL), 0)
        == group * (GL // CH) + lax.broadcasted_iota(jnp.int32, (heads, GL), 1) // CH
    ).astype(BF)
    hi, mid, low = split3(spike_ref[...])
    over = ((0,), (0,))
    burst = dot(hi, spread, over) + dot(mid, spread, over) + dot(low, spread, over)
    return keys, burst - keys * poly


def running_sum(logs, length):
    lower = tri(length).astype(BF)
    out = []
    for b in range(logs.shape[0] // length):
        hi, low = split2(logs[b * length : (b + 1) * length])
        out.append(dot(lower, hi) + dot(lower, low))
    return out


def states_kernel(f_ref, v_ref, floor_ref, spike_ref, pack_ref):
    group = pl.program_id(0)
    keys, logs = keys_and_logs(f_ref, floor_ref, spike_ref, group)
    parts = running_sum(logs, 128)
    after = jnp.zeros((1, GL), F32)
    acc = jnp.zeros((GL, GL), F32)
    for b in reversed(range(len(parts))):
        close = parts[b][127:128]
        kc = (keys[b * 128 : (b + 1) * 128] * jnp.exp(after + close - parts[b])).astype(BF)
        acc = acc + dot(v_ref[b * 128 : (b + 1) * 128, :], kc, ((0,), (0,)))
        after = after + close
    acc = jnp.where(same_head(GL, GL), acc, 0.0)
    compact = acc[0:64] + acc[64:128] + acc[128:192] + acc[192:256]
    pack_ref[0:64, :] = compact.astype(BF)
    hi, mid, low = split3(after)
    row = lax.broadcasted_iota(jnp.int32, (16, GL), 0)
    tail = jnp.where(row == 0, hi.astype(F32), 0.0)
    tail = jnp.where(row == 1, mid.astype(F32), tail)
    tail = jnp.where(row == 2, low.astype(F32), tail)
    pack_ref[64:80, :] = tail.astype(BF)


def inside_kernel(q_ref, f_ref, v_ref, floor_ref, spike_ref, out_ref, qrun_ref):
    group = pl.program_id(0)
    keys, logs = keys_and_logs(f_ref, floor_ref, spike_ref, group)
    parts = running_sum(logs, BLK)
    q = silu(q_ref[...].astype(F32))
    head_mask = same_head(GL, GL)
    lane = lax.broadcasted_iota(jnp.int32, (BLK, GL), 1)
    causal = (lane % CH) <= lax.broadcasted_iota(jnp.int32, (BLK, GL), 0)
    before = jnp.zeros((1, GL), F32)
    state = jnp.zeros((GL, GL), F32)
    zero = jnp.zeros((GL, GL), BF)
    for b in range(len(parts)):
        rows = slice(b * BLK, (b + 1) * BLK)
        cum = parts[b]
        close = cum[BLK - 1 : BLK]
        k = keys[rows]
        grow = jnp.exp(-cum)
        qd = q[rows] * jnp.exp(cum)
        qrun_ref[rows, :] = (qd * jnp.exp(before)).astype(BF)
        qd = qd.astype(BF)
        k = k * grow
        kg = k.astype(BF)
        v = v_ref[rows, :]
        k4 = jnp.where(head_mask, jnp.concatenate([kg] * 4, axis=0), zero)
        v4 = jnp.where(head_mask, jnp.concatenate([v] * 4, axis=0), zero)
        scores = dot(qd, k4, ((1,), (1,)))
        scores = jnp.where(causal, scores, 0.0).astype(BF)
        out = dot(scores, v4)
        if b > 0:
            out = out + dot(qd, state.astype(BF), ((1,), (1,)))
        out_ref[rows, :] = out
        if b + 1 < len(parts):
            kc = (k * jnp.exp(close)).astype(BF)
            add = jnp.where(head_mask, dot(v, kc, ((0,), (0,))), 0.0)
            state = jnp.exp(close) * state + add
        before = before + close


def total_of(pack_ref):
    return (
        pack_ref[64:65, :].astype(F32)
        + pack_ref[65:66, :].astype(F32)
        + pack_ref[66:67, :].astype(F32)
    )


def row_kernel(pos_ref, own_ref, one_ref, two_ref, three_ref, row_ref, before_ref, btot_ref):
    here = pos_ref[0]
    width = own_ref.shape[1]
    state = jnp.zeros((CH, width), F32)
    total = jnp.zeros((1, width), F32)
    pieces = ((3, three_ref), (2, two_ref), (1, one_ref))
    for n, ref in pieces:
        use = n <= here
        t = jnp.where(use, total_of(ref), 0.0)
        state = jnp.exp(t) * state + jnp.where(use, ref[0:64, :].astype(F32), 0.0)
        total = total + t
    before_ref[...] = state
    btot_ref[...] = jnp.broadcast_to(total, (8, width))
    t = total_of(own_ref)
    state = jnp.exp(t) * state + own_ref[0:64, :].astype(F32)
    total = total + t
    for n, ref in pieces:
        use = n > here
        t = jnp.where(use, total_of(ref), 0.0)
        state = jnp.exp(t) * state + jnp.where(use, ref[0:64, :].astype(F32), 0.0)
        total = total + t
    row_ref[0:64, :] = state.astype(BF)
    hi, mid, low = split3(total)
    row = lax.broadcasted_iota(jnp.int32, (16, width), 0)
    tail = jnp.where(row == 0, hi.astype(F32), 0.0)
    tail = jnp.where(row == 1, mid.astype(F32), tail)
    tail = jnp.where(row == 2, low.astype(F32), tail)
    row_ref[64:80, :] = tail.astype(BF)


def mix_kernel(
    tok_steps,
    cap,
    pos_ref,
    out_ref,
    qrun_ref,
    gate_ref,
    res_ref,
    before_ref,
    btot_ref,
    one_ref,
    two_ref,
    three_ref,
    *refs,
):
    wmine = refs[0:4]
    wother = refs[4:8]
    scale_ref, routes_ref, upd_ref, send_ref, w_s, state_s, norm_s, pos_s, sems = refs[8:]

    step = pl.program_id(0)
    width = gate_ref.shape[1]
    groups = width // GL
    tok_rows = routes_ref.shape[1]
    rows = gate_ref.shape[0]

    piece = wmine[0].shape[0]

    def weight_copies():
        for n in range(4):
            src = (pos_ref[1] + 4 - n) % 4
            for i, (ref, core) in enumerate(((wmine[n], pos_ref[2]), (wother[n], 1 - pos_ref[2]))):
                where = pl.ds(pl.multiple_of((2 * src + core) * piece, piece), piece)
                yield pltpu.make_async_copy(ref, w_s.at[where], sems.at[2 * n + i])

    @pl.when(step == 0)
    def _():
        for c in weight_copies():
            c.start()
        here = pos_ref[0]
        state = jnp.zeros((CH, width), F32)
        for n, ref in ((3, three_ref), (2, two_ref), (1, one_ref)):
            use = n <= here
            t = jnp.where(use, total_of(ref), 0.0)
            state = jnp.exp(t) * state + jnp.where(use, ref[0:64, :].astype(F32), 0.0)
        state = (jnp.exp(btot_ref[0:1, :]) * state + before_ref[...]).astype(BF)
        mask = same_head(GL, GL)
        for g in range(groups):
            one = state[:, g * GL : (g + 1) * GL]
            state_s[g] = jnp.where(mask, jnp.concatenate([one] * 4, axis=0), jnp.zeros((GL, GL), BF))
        experts = pos_s.shape[0]
        e = lax.broadcasted_iota(jnp.int32, (experts, tok_rows), 0)
        member = (e == routes_ref[0:1, :]) | (e == routes_ref[1:2, :])
        mem = jnp.where(member, 1.0, 0.0)
        strict = (
            lax.broadcasted_iota(jnp.int32, (tok_rows, tok_rows), 0)
            < lax.broadcasted_iota(jnp.int32, (tok_rows, tok_rows), 1)
        ).astype(BF)
        place = dot(mem.astype(BF), strict)
        pos_s[...] = jnp.where(member, place.astype(jnp.int32), -1)

    @pl.when(step < tok_steps)
    def _():
        ones = jnp.where(same_head(GL, GL), 1.0, 0.0).astype(BF)
        mixed = []
        for g in range(groups):
            lanes = slice(g * GL, (g + 1) * GL)
            o = out_ref[:, lanes] + dot(qrun_ref[:, lanes], state_s[g], ((1,), (1,)))
            hi, low = split2(o * o)
            mean = (dot(hi, ones) + dot(low, ones)) * (1.0 / CH)
            gate = silu(gate_ref[:, lanes].astype(F32))
            mixed.append((o * lax.rsqrt(mean + 1e-06) * gate).astype(BF))
        mixed = jnp.concatenate(mixed, axis=1)

        @pl.when(step == 0)
        def _():
            for c in weight_copies():
                c.wait()

        upd = (res_ref[...].astype(F32) + dot(mixed, w_s[...])).astype(BF)
        upd_ref[...] = upd
        wide = upd.astype(F32)
        mean = jnp.mean(wide * wide, axis=-1, keepdims=True)
        norm = (wide * lax.rsqrt(mean + 1e-06) * scale_ref[...]).astype(BF)
        norm_s[pl.ds(step * rows, rows), :] = norm

    @pl.when(step >= tok_steps)
    def _():
        per = send_ref.shape[0] // cap
        picks = []
        for i in range(per):
            place = pos_s[pl.ds((step - tok_steps) * per + i, 1), :]
            c = lax.broadcasted_iota(jnp.int32, (cap, tok_rows), 0)
            picks.append(jnp.where(c == place, 1.0, 0.0).astype(BF))
        send_ref[...] = dot(jnp.concatenate(picks, axis=0), norm_s[...]).astype(BF)


def serve_kernel(
    first, parts, x_ref, wg_ref, wu_ref, wd_ref, out_ref, x_s, wg_s, wu_s, wd_s, hid_s, out_s, sems, out_sems
):
    srcs, size, model = x_s.shape
    hid = hid_s.shape[1]
    steps = 4
    hb = hid // steps
    ob = model // steps
    per = srcs // parts
    rows = per * size

    def x_copy(m):
        lo = m * per
        return pltpu.make_async_copy(
            x_ref.at[pl.ds(lo, per), pl.ds(first, size), :], x_s.at[pl.ds(lo, per)], sems.at[m]
        )

    def w_copy(which, n):
        src, dst, cols = ((wg_ref, wg_s, hb), (wu_ref, wu_s, hb), (wd_ref, wd_s, ob))[which]
        lanes = pl.ds(n * cols, cols)
        return pltpu.make_async_copy(
            src.at[0, :, lanes], dst.at[:, lanes], sems.at[parts + which * steps + n]
        )

    def out_copy(m, n):
        lanes = pl.ds(n * ob, ob)
        return pltpu.make_async_copy(
            out_s.at[pl.ds(m * per, per), :, lanes],
            out_ref.at[pl.ds(m * per, per), :, lanes],
            out_sems.at[m * steps + n],
        )

    x_copy(0).start()
    w_copy(0, 0).start()
    w_copy(1, 0).start()
    for m in range(1, parts):
        x_copy(m).start()
    x_copy(0).wait()
    w_copy(0, 0).wait()
    w_copy(1, 0).wait()
    for n in range(1, steps):
        w_copy(0, n).start()
        w_copy(1, n).start()
    for n in range(steps):
        w_copy(2, n).start()
    for n in range(steps):
        lanes = slice(n * hb, (n + 1) * hb)
        if n > 0:
            w_copy(0, n).wait()
            w_copy(1, n).wait()
        for m in range(parts):
            if n == 0 and m > 0:
                x_copy(m).wait()
            x = x_s[m * per : (m + 1) * per].reshape(rows, model)
            hidden = silu(dot(x, wg_s[:, lanes])) * dot(x, wu_s[:, lanes])
            hid_s[m * rows : (m + 1) * rows, lanes] = hidden.astype(BF)
    for n in range(steps):
        lanes = slice(n * ob, (n + 1) * ob)
        w_copy(2, n).wait()
        for m in range(parts):
            got = dot(hid_s[m * rows : (m + 1) * rows, :], wd_s[:, lanes]).astype(BF)
            out_s[m * per : (m + 1) * per, :, lanes] = got.reshape(per, size, ob)
            out_copy(m, n).start()
    for n in range(steps):
        for m in range(parts):
            out_copy(m, n).wait()


def serve_rest_kernel(
    first, parts, x_ref, wg_ref, wu_ref, wd_ref, out_ref, x_s, wd_s, hid_s, out_s, sems, wd_sems, out_sems
):
    srcs, size, model = x_s.shape
    hid = hid_s.shape[1]
    steps = 4
    hb = hid // steps
    ob = model // steps
    per = srcs // parts
    rows = per * size

    def x_copy(m):
        lo = m * per
        return pltpu.make_async_copy(
            x_ref.at[pl.ds(lo, per), pl.ds(first, size), :], x_s.at[pl.ds(lo, per)], sems.at[m]
        )

    def wd_copy(n):
        lanes = pl.ds(n * ob, ob)
        return pltpu.make_async_copy(wd_ref.at[0, :, lanes], wd_s.at[:, lanes], wd_sems.at[n])

    def out_copy(m, n):
        lanes = pl.ds(n * ob, ob)
        return pltpu.make_async_copy(
            out_s.at[pl.ds(m * per, per), :, lanes],
            out_ref.at[pl.ds(m * per, per), :, lanes],
            out_sems.at[m * steps + n],
        )

    for m in range(parts):
        x_copy(m).start()
    for n in range(steps):
        wd_copy(n).start()
    for n in range(steps):
        lanes = slice(n * hb, (n + 1) * hb)
        for m in range(parts):
            if n == 0:
                x_copy(m).wait()
            x = x_s[m * per : (m + 1) * per].reshape(rows, model)
            hidden = silu(dot(x, wg_ref[0, :, lanes])) * dot(x, wu_ref[0, :, lanes])
            hid_s[m * rows : (m + 1) * rows, lanes] = hidden.astype(BF)
    for n in range(steps):
        lanes = slice(n * ob, (n + 1) * ob)
        wd_copy(n).wait()
        for m in range(parts):
            got = dot(hid_s[m * rows : (m + 1) * rows, :], wd_s[:, lanes]).astype(BF)
            out_s[m * per : (m + 1) * per, :, lanes] = got.reshape(per, size, ob)
            out_copy(m, n).start()
    for n in range(steps):
        for m in range(parts):
            out_copy(m, n).wait()


def weights_kernel(main, routes_ref, wt_ref, main_ref, rest_ref):
    tok_rows = routes_ref.shape[1]
    experts = main_ref.shape[1] // main
    routes = jnp.transpose(routes_ref[...])
    wts = jnp.transpose(wt_ref[...])
    lane = lax.broadcasted_iota(jnp.int32, (tok_rows, 128), 1)
    strict = (
        lax.broadcasted_iota(jnp.int32, (tok_rows, tok_rows), 0)
        > lax.broadcasted_iota(jnp.int32, (tok_rows, tok_rows), 1)
    ).astype(BF)
    ones = [lane == routes[:, k : k + 1] for k in range(2)]
    place = dot(strict, jnp.where(ones[0] | ones[1], 1.0, 0.0).astype(BF))
    for ref, base in ((main_ref, 0), (rest_ref, main)):
        size = ref.shape[1] // experts
        j = lax.broadcasted_iota(jnp.int32, ref.shape, 1)
        weight = jnp.zeros(ref.shape, F32)
        for k in range(2):
            p = jnp.sum(jnp.where(ones[k], place, 0.0), axis=1, keepdims=True).astype(jnp.int32)
            p = p - base
            slot = jnp.where((p >= 0) & (p < size), routes[:, k : k + 1] * size + p, -1)
            weight = jnp.where(j == slot, wts[:, k : k + 1], weight)
        ref[...] = weight.astype(BF)


def combine_kernel(main_ref, rest_ref, got_ref, got_rest_ref, upd_ref, out_ref, out_s, sems):
    steps = sems.shape[0]
    blk = out_s.shape[1] // steps

    def out_copy(n):
        lanes = pl.ds(n * blk, blk)
        return pltpu.make_async_copy(out_s.at[:, lanes], out_ref.at[:, lanes], sems.at[n])

    for n in range(steps):
        lanes = slice(n * blk, (n + 1) * blk)
        total = dot(main_ref[...], got_ref[:, lanes]) + dot(rest_ref[...], got_rest_ref[:, lanes])
        out_s[:, lanes] = (upd_ref[:, lanes].astype(F32) + total).astype(out_s.dtype)
        out_copy(n).start()
    for n in range(steps):
        out_copy(n).wait()


def cost(us):
    return pl.CostEstimate(flops=int(us * 5e8), bytes_accessed=int(us * 1e6), transcendentals=0)


def ring(n, size=4):
    return [(i, (i + n) % size) for i in range(size)]


def per_device(
    query_weight,
    forget_preactivation,
    written_input,
    output_gate_logit,
    forget_floor,
    extra_log_decay,
    residual,
    output_weight,
    norm_scale_vector,
    expert_gate_weight,
    expert_up_weight,
    expert_down_weight,
    routes,
    routing_weight,
):
    _, tok, width = query_weight.shape
    model = output_weight.shape[1]
    heads = width // CH
    groups = width // GL
    experts = lax.axis_size(SP)
    cap = 4 * tok // experts
    main = cap * 5 // 6
    rest = cap - main
    z = lax.axis_index("sp_0")
    y = lax.axis_index("sp_1")
    x = lax.axis_index("x")
    core = lax.axis_index("c")

    spikes = lax.dynamic_slice_in_dim(extra_log_decay[0].T, lax.axis_index(SP) * tok, tok, 1)
    q, f, v, gate = (
        a.reshape(tok, width)
        for a in (query_weight, forget_preactivation, written_input, output_gate_logit)
    )
    floor = forget_floor.reshape(1, width)
    scale = norm_scale_vector.reshape(1, model)
    res = residual.reshape(tok, model)

    mine = output_weight
    wmine = [lax.ppermute(mine, "x", ring(n)) for n in (1, 2, 3)]

    tall = pl.BlockSpec((tok, GL), lambda g: (0, g))
    flat = pl.BlockSpec((1, GL), lambda g: (0, g))
    whole = pl.BlockSpec((heads, tok), lambda g: (0, 0))
    pack = pl.pallas_call(
        states_kernel,
        grid=(groups,),
        in_specs=[tall, tall, flat, whole],
        out_specs=pl.BlockSpec((PACK, GL), lambda g: (0, g)),
        out_shape=jax.ShapeDtypeStruct((PACK, width), BF),
        cost_estimate=cost(7),
        compiler_params=pltpu.CompilerParams(vmem_limit_bytes=66 * 1000 * 1000),
        name="states",
    )(f, v, floor, spikes)

    along_y = [lax.ppermute(pack, "sp_1", ring(n)) for n in (1, 2, 3)]


    vm = pl.BlockSpec(memory_space=pltpu.VMEM)
    sm = pl.BlockSpec(memory_space=pltpu.SMEM)

    inside, qrun = pl.pallas_call(
        inside_kernel,
        grid=(groups,),
        in_specs=[tall, tall, tall, flat, whole],
        out_specs=[tall, tall],
        out_shape=[jax.ShapeDtypeStruct((tok, width), F32), jax.ShapeDtypeStruct((tok, width), BF)],
        cost_estimate=cost(8),
        compiler_params=pltpu.CompilerParams(vmem_limit_bytes=66 * 1000 * 1000),
        name="inside",
    )(q, f, v, floor, spikes)

    row, before, btot = pl.pallas_call(
        row_kernel,
        in_specs=[sm, vm, vm, vm, vm],
        out_specs=[vm, vm, vm],
        out_shape=[
            jax.ShapeDtypeStruct((PACK, width), BF),
            jax.ShapeDtypeStruct((CH, width), F32),
            jax.ShapeDtypeStruct((8, width), F32),
        ],
        cost_estimate=cost(2),
        compiler_params=pltpu.CompilerParams(vmem_limit_bytes=66 * 1000 * 1000),
        name="row",
    )(y.astype(jnp.int32).reshape(1), pack, *along_y)

    along_z = [lax.ppermute(row, "sp_0", ring(n)) for n in (1, 2, 3)]

    wmine, row = lax.optimization_barrier((wmine, row))
    wmine = [mine] + wmine
    wother = [lax.ppermute(p, "c", ring(1, 2)) for p in wmine]

    route_rows = jnp.pad(routes[0].T, ((0, 6), (0, 0)), constant_values=-1)
    wt_rows = jnp.pad(routing_weight[0].T, ((0, 6), (0, 0)))
    route_rows, wt_rows, row = lax.optimization_barrier((route_rows, wt_rows, row))
    weights_main, weights_rest = pl.pallas_call(
        functools.partial(weights_kernel, main),
        in_specs=[vm, vm],
        out_specs=[vm, vm],
        out_shape=[
            jax.ShapeDtypeStruct((tok, experts * main), BF),
            jax.ShapeDtypeStruct((tok, experts * rest), BF),
        ],
        cost_estimate=cost(2),
        compiler_params=pltpu.CompilerParams(vmem_limit_bytes=66 * 1000 * 1000),
        name="weights",
    )(route_rows, wt_rows)


    place = jnp.stack([z, x, core]).astype(jnp.int32)
    tok_steps = 2
    rows = tok // tok_steps
    send_steps = 4
    send_rows = experts * cap // send_steps
    clip = lambda i: jnp.minimum(i, tok_steps - 1)
    tok_w = pl.BlockSpec((rows, width), lambda i: (clip(i), 0))
    tok_m = pl.BlockSpec((rows, model), lambda i: (clip(i), 0))
    full = lambda a: pl.BlockSpec(a.shape, lambda i: (0,) * a.ndim)


    updated, send = pl.pallas_call(
        functools.partial(mix_kernel, tok_steps, cap),
        grid=(tok_steps + send_steps,),
        in_specs=[
            sm,
            tok_w,
            tok_w,
            tok_w,
            tok_m,
            full(before),
            full(btot),
            full(row),
            full(row),
            full(row),
            *[pl.BlockSpec(memory_space=pl.ANY)] * 8,
            full(scale),
            full(route_rows),
        ],
        out_specs=[
            tok_m,
            pl.BlockSpec((send_rows, model), lambda i: (jnp.maximum(i - tok_steps, 0), 0)),
        ],
        out_shape=[
            jax.ShapeDtypeStruct((tok, model), BF),
            jax.ShapeDtypeStruct((experts * cap, model), BF),
        ],
        scratch_shapes=[
            pltpu.VMEM((width, model), BF),
            pltpu.VMEM((groups, GL, GL), BF),
            pltpu.VMEM((tok, model), BF),
            pltpu.VMEM((experts, tok), jnp.int32),
            pltpu.SemaphoreType.DMA((8,)),
        ],
        compiler_params=pltpu.CompilerParams(vmem_limit_bytes=66 * 1000 * 1000),
        cost_estimate=cost(12),
        name="mix",
    )(place, inside, qrun, gate, res, before, btot, *along_z, *wmine, *wother, scale, route_rows)

    def exchange(a):
        return lax.all_to_all(a, SP, split_axis=0, concat_axis=0, tiled=True)

    hid = expert_gate_weight.shape[2]
    anywhere = pl.BlockSpec(memory_space=pl.ANY)

    dma = lambda n: pltpu.SemaphoreType.DMA((n,))

    def serve(kernel, arrived, first, size, parts, scratch, specs, limit, us):
        return pl.pallas_call(
            functools.partial(kernel, first, parts),
            in_specs=[anywhere, *specs],
            out_specs=anywhere,
            out_shape=jax.ShapeDtypeStruct((experts, size, model), BF),
            scratch_shapes=[
                pltpu.VMEM((experts, size, model), BF),
                *[pltpu.VMEM(shape, BF) for shape in scratch],
                pltpu.VMEM((experts * size, hid), BF),
                pltpu.VMEM((experts, size, model), BF),
                *([dma(parts), dma(4)] if kernel is serve_rest_kernel else [dma(parts + 12)]),
                dma(parts * 4),
            ],
            compiler_params=pltpu.CompilerParams(vmem_limit_bytes=limit * 1024 * 1024),
            cost_estimate=cost(us),
            name="serve",
        )(arrived, expert_gate_weight, expert_up_weight, expert_down_weight)

    def serve_main(arrived):
        scratch = [(model, hid), (model, hid), (hid, model)]
        return serve(serve_kernel, arrived, 0, main, 2, scratch, [anywhere] * 3, 50, 20)

    def serve_rest(arrived):
        specs = [vm, vm, anywhere]
        return serve(serve_rest_kernel, arrived, main, rest, 1, [(hid, model)], specs, 36, 5)

    arrived = exchange(send.reshape(experts, cap, model))
    served_rest = serve_rest(arrived)
    got_rest = exchange(served_rest)

    got = exchange(serve_main(arrived))

    layer_out = pl.pallas_call(
        combine_kernel,
        in_specs=[vm] * 5,
        out_specs=anywhere,
        out_shape=jax.ShapeDtypeStruct((tok, model), BF),
        scratch_shapes=[pltpu.VMEM((tok, model), BF), pltpu.SemaphoreType.DMA((4,))],
        compiler_params=pltpu.CompilerParams(vmem_limit_bytes=40 * 1024 * 1024),
        cost_estimate=cost(4),
        name="combine",
    )(
        weights_main,
        weights_rest,
        got.reshape(experts * main, model),
        got_rest.reshape(experts * rest, model),
        updated,
    )
    return layer_out.reshape(1, tok, model)


def solution(mesh):
    torus = Mesh(
        mesh.devices.reshape(4, 4, 4, mesh.shape["dp"] // 4), ("sp_0", "sp_1", "x", "c")
    )
    return jax.shard_map(
        per_device,
        mesh=torus,
        in_specs=(
            P(DP, SP, None),
            P(DP, SP, None),
            P(DP, SP, None),
            P(DP, SP, None),
            P(),
            P(DP, None, None),
            P(DP, SP, None),
            P(DP, None),
            P(),
            P(SP, None, None),
            P(SP, None, None),
            P(SP, None, None),
            P(DP, SP, None),
            P(DP, SP, None),
        ),
        out_specs=P(DP, SP, None),
        check_vma=False,
    )
```

```python
import functools

import jax
import jax.numpy as jnp
from jax import lax
from jax.experimental import pallas as pl
from jax.experimental.pallas import tpu as pltpu
from jax.sharding import Mesh
from jax.sharding import PartitionSpec as P

CH = 64
BLK = 64
GL = 256
SP = ("sp_0", "sp_1")
DP = ("x", "c")
PACK = 72
F32 = jnp.float32
BF = jnp.bfloat16


def dot(a, b, dims=((1,), (0,))):
    return lax.dot_general(a, b, (dims, ((), ())), preferred_element_type=F32)


def split3(v):
    hi = v.astype(BF)
    rest = v - hi.astype(F32)
    mid = rest.astype(BF)
    low = (rest - mid.astype(F32)).astype(BF)
    return hi, mid, low


def split2(v):
    hi = v.astype(BF)
    return hi, (v - hi.astype(F32)).astype(BF)


def tri(n):
    return (
        lax.broadcasted_iota(jnp.int32, (n, n), 0) >= lax.broadcasted_iota(jnp.int32, (n, n), 1)
    )


def same_head(rows, lanes):
    return (
        lax.broadcasted_iota(jnp.int32, (rows, lanes), 0) // CH
        == lax.broadcasted_iota(jnp.int32, (rows, lanes), 1) // CH
    )


def silu(v):
    return v / (1.0 + jnp.exp(-v))


def keys_and_logs(f_ref, floor_ref, spike_ref, group):
    f = f_ref[...].astype(F32)
    keys = (1.0 - floor_ref[...]) / (1.0 + jnp.exp(f))
    poly = jnp.full_like(keys, 1.0 / 7.0)
    for n in range(6, 0, -1):
        poly = poly * keys + 1.0 / n
    heads = spike_ref.shape[0]
    spread = (
        lax.broadcasted_iota(jnp.int32, (heads, GL), 0)
        == group * (GL // CH) + lax.broadcasted_iota(jnp.int32, (heads, GL), 1) // CH
    ).astype(BF)
    hi, mid, low = split3(spike_ref[...])
    over = ((0,), (0,))
    burst = dot(hi, spread, over) + dot(mid, spread, over) + dot(low, spread, over)
    return keys, burst - keys * poly


def running_sum(logs, length):
    lower = tri(length).astype(BF)
    out = []
    for b in range(logs.shape[0] // length):
        hi, low = split2(logs[b * length : (b + 1) * length])
        out.append(dot(lower, hi) + dot(lower, low))
    return out


def states_kernel(f_ref, v_ref, floor_ref, spike_ref, pack_ref):
    group = pl.program_id(0)
    keys, logs = keys_and_logs(f_ref, floor_ref, spike_ref, group)
    parts = running_sum(logs, 128)
    after = jnp.zeros((1, GL), F32)
    acc = jnp.zeros((GL, GL), F32)
    for b in reversed(range(len(parts))):
        close = parts[b][127:128]
        kc = (keys[b * 128 : (b + 1) * 128] * jnp.exp(after + close - parts[b])).astype(BF)
        acc = acc + dot(v_ref[b * 128 : (b + 1) * 128, :], kc, ((0,), (0,)))
        after = after + close
    acc = jnp.where(same_head(GL, GL), acc, 0.0)
    compact = acc[0:64] + acc[64:128] + acc[128:192] + acc[192:256]
    pack_ref[0:64, :] = compact.astype(BF)
    hi, mid, low = split3(after)
    row = lax.broadcasted_iota(jnp.int32, (8, GL), 0)
    tail = jnp.where(row == 0, hi.astype(F32), 0.0)
    tail = jnp.where(row == 1, mid.astype(F32), tail)
    tail = jnp.where(row == 2, low.astype(F32), tail)
    pack_ref[64:72, :] = tail.astype(BF)


def inside_kernel(q_ref, f_ref, v_ref, floor_ref, spike_ref, out_ref, qrun_ref):
    group = pl.program_id(0)
    keys, logs = keys_and_logs(f_ref, floor_ref, spike_ref, group)
    parts = running_sum(logs, BLK)
    q = silu(q_ref[...].astype(F32))
    head_mask = same_head(GL, GL)
    lane = lax.broadcasted_iota(jnp.int32, (BLK, GL), 1)
    causal = (lane % CH) <= lax.broadcasted_iota(jnp.int32, (BLK, GL), 0)
    before = jnp.zeros((1, GL), F32)
    state = jnp.zeros((GL, GL), F32)
    zero = jnp.zeros((GL, GL), BF)
    for b in range(len(parts)):
        rows = slice(b * BLK, (b + 1) * BLK)
        cum = parts[b]
        close = cum[BLK - 1 : BLK]
        k = keys[rows]
        grow = jnp.exp(-cum)
        qd = q[rows] * jnp.exp(cum)
        qrun_ref[rows, :] = (qd * jnp.exp(before)).astype(BF)
        qd = qd.astype(BF)
        k = k * grow
        kg = k.astype(BF)
        v = v_ref[rows, :]
        k4 = jnp.where(head_mask, jnp.concatenate([kg] * 4, axis=0), zero)
        v4 = jnp.where(head_mask, jnp.concatenate([v] * 4, axis=0), zero)
        scores = dot(qd, k4, ((1,), (1,)))
        scores = jnp.where(causal, scores, 0.0).astype(BF)
        out = dot(scores, v4)
        if b > 0:
            out = out + dot(qd, state.astype(BF), ((1,), (1,)))
        out_ref[rows, :] = out
        if b + 1 < len(parts):
            kc = (k * jnp.exp(close)).astype(BF)
            add = jnp.where(head_mask, dot(v, kc, ((0,), (0,))), 0.0)
            state = jnp.exp(close) * state + add
        before = before + close


def total_of(pack_ref):
    return (
        pack_ref[64:65, :].astype(F32)
        + pack_ref[65:66, :].astype(F32)
        + pack_ref[66:67, :].astype(F32)
    )


def row_kernel(pos_ref, own_ref, one_ref, two_ref, three_ref, row_ref, before_ref, btot_ref):
    here = pos_ref[0]
    width = own_ref.shape[1]
    state = jnp.zeros((CH, width), F32)
    total = jnp.zeros((1, width), F32)
    pieces = ((3, three_ref), (2, two_ref), (1, one_ref))
    for n, ref in pieces:
        use = n <= here
        t = jnp.where(use, total_of(ref), 0.0)
        state = jnp.exp(t) * state + jnp.where(use, ref[0:64, :].astype(F32), 0.0)
        total = total + t
    before_ref[...] = state
    btot_ref[...] = jnp.broadcast_to(total, (8, width))
    t = total_of(own_ref)
    state = jnp.exp(t) * state + own_ref[0:64, :].astype(F32)
    total = total + t
    for n, ref in pieces:
        use = n > here
        t = jnp.where(use, total_of(ref), 0.0)
        state = jnp.exp(t) * state + jnp.where(use, ref[0:64, :].astype(F32), 0.0)
        total = total + t
    row_ref[0:64, :] = state.astype(BF)
    hi, mid, low = split3(total)
    row = lax.broadcasted_iota(jnp.int32, (8, width), 0)
    tail = jnp.where(row == 0, hi.astype(F32), 0.0)
    tail = jnp.where(row == 1, mid.astype(F32), tail)
    tail = jnp.where(row == 2, low.astype(F32), tail)
    row_ref[64:72, :] = tail.astype(BF)


def mix_kernel(
    tok_steps,
    cap,
    pos_ref,
    out_ref,
    qrun_ref,
    gate_ref,
    res_ref,
    before_ref,
    btot_ref,
    one_ref,
    two_ref,
    three_ref,
    *refs,
):
    wmine = refs[0:4]
    wother = refs[4:8]
    scale_ref, routes_ref, upd_ref, send_ref, w_s, state_s, norm_s, pos_s, sems = refs[8:]

    step = pl.program_id(0)
    width = gate_ref.shape[1]
    groups = width // GL
    tok_rows = routes_ref.shape[1]
    rows = gate_ref.shape[0]

    piece = wmine[0].shape[0]

    def weight_copies():
        for n in range(4):
            src = (pos_ref[1] + 4 - n) % 4
            for i, (ref, core) in enumerate(((wmine[n], pos_ref[2]), (wother[n], 1 - pos_ref[2]))):
                where = pl.ds(pl.multiple_of((2 * src + core) * piece, piece), piece)
                yield pltpu.make_async_copy(ref, w_s.at[where], sems.at[2 * n + i])

    @pl.when(step == 0)
    def _():
        for c in weight_copies():
            c.start()
        here = pos_ref[0]
        state = jnp.zeros((CH, width), F32)
        for n, ref in ((3, three_ref), (2, two_ref), (1, one_ref)):
            use = n <= here
            t = jnp.where(use, total_of(ref), 0.0)
            state = jnp.exp(t) * state + jnp.where(use, ref[0:64, :].astype(F32), 0.0)
        state = (jnp.exp(btot_ref[0:1, :]) * state + before_ref[...]).astype(BF)
        mask = same_head(GL, GL)
        for g in range(groups):
            one = state[:, g * GL : (g + 1) * GL]
            state_s[g] = jnp.where(mask, jnp.concatenate([one] * 4, axis=0), jnp.zeros((GL, GL), BF))
        experts = pos_s.shape[0]
        e = lax.broadcasted_iota(jnp.int32, (experts, tok_rows), 0)
        member = (e == routes_ref[0:1, :]) | (e == routes_ref[1:2, :])
        mem = jnp.where(member, 1.0, 0.0)
        strict = (
            lax.broadcasted_iota(jnp.int32, (tok_rows, tok_rows), 0)
            < lax.broadcasted_iota(jnp.int32, (tok_rows, tok_rows), 1)
        ).astype(BF)
        place = dot(mem.astype(BF), strict)
        pos_s[...] = jnp.where(member, place.astype(jnp.int32), -1)

    @pl.when(step < tok_steps)
    def _():
        ones = jnp.where(same_head(GL, GL), 1.0, 0.0).astype(BF)
        mixed = []
        for g in range(groups):
            lanes = slice(g * GL, (g + 1) * GL)
            o = out_ref[:, lanes] + dot(qrun_ref[:, lanes], state_s[g], ((1,), (1,)))
            hi, low = split2(o * o)
            mean = (dot(hi, ones) + dot(low, ones)) * (1.0 / CH)
            gate = silu(gate_ref[:, lanes].astype(F32))
            mixed.append((o * lax.rsqrt(mean + 1e-06) * gate).astype(BF))
        mixed = jnp.concatenate(mixed, axis=1)

        @pl.when(step == 0)
        def _():
            for c in weight_copies():
                c.wait()

        upd = (res_ref[...].astype(F32) + dot(mixed, w_s[...])).astype(BF)
        upd_ref[...] = upd
        wide = upd.astype(F32)
        mean = jnp.mean(wide * wide, axis=-1, keepdims=True)
        norm = (wide * lax.rsqrt(mean + 1e-06) * scale_ref[...]).astype(BF)
        norm_s[pl.ds(step * rows, rows), :] = norm

    @pl.when(step >= tok_steps)
    def _():
        per = send_ref.shape[0] // cap
        picks = []
        for i in range(per):
            place = pos_s[pl.ds((step - tok_steps) * per + i, 1), :]
            c = lax.broadcasted_iota(jnp.int32, (cap, tok_rows), 0)
            picks.append(jnp.where(c == place, 1.0, 0.0).astype(BF))
        send_ref[...] = dot(jnp.concatenate(picks, axis=0), norm_s[...]).astype(BF)


def serve_kernel(
    first, parts, x_ref, wg_ref, wu_ref, wd_ref, out_ref, x_s, wg_s, wu_s, wd_s, hid_s, out_s, sems, out_sems
):
    srcs, size, model = x_s.shape
    hid = hid_s.shape[1]
    steps = 4
    hb = hid // steps
    ob = model // steps
    per = srcs // parts
    rows = per * size

    def x_copy(m):
        lo = m * per
        return pltpu.make_async_copy(
            x_ref.at[pl.ds(lo, per), pl.ds(first, size), :], x_s.at[pl.ds(lo, per)], sems.at[m]
        )

    def w_copy(which, n):
        src, dst, cols = ((wg_ref, wg_s, hb), (wu_ref, wu_s, hb), (wd_ref, wd_s, ob))[which]
        lanes = pl.ds(n * cols, cols)
        return pltpu.make_async_copy(
            src.at[0, :, lanes], dst.at[:, lanes], sems.at[parts + which * steps + n]
        )

    def out_copy(m, n):
        lanes = pl.ds(n * ob, ob)
        return pltpu.make_async_copy(
            out_s.at[pl.ds(m * per, per), :, lanes],
            out_ref.at[pl.ds(m * per, per), :, lanes],
            out_sems.at[m * steps + n],
        )

    x_copy(0).start()
    w_copy(0, 0).start()
    w_copy(1, 0).start()
    for m in range(1, parts):
        x_copy(m).start()
    x_copy(0).wait()
    w_copy(0, 0).wait()
    w_copy(1, 0).wait()
    for n in range(1, steps):
        w_copy(0, n).start()
        w_copy(1, n).start()
    for n in range(steps):
        w_copy(2, n).start()
    for n in range(steps):
        lanes = slice(n * hb, (n + 1) * hb)
        if n > 0:
            w_copy(0, n).wait()
            w_copy(1, n).wait()
        for m in range(parts):
            if n == 0 and m > 0:
                x_copy(m).wait()
            x = x_s[m * per : (m + 1) * per].reshape(rows, model)
            hidden = silu(dot(x, wg_s[:, lanes])) * dot(x, wu_s[:, lanes])
            hid_s[m * rows : (m + 1) * rows, lanes] = hidden.astype(BF)
    for n in range(steps):
        lanes = slice(n * ob, (n + 1) * ob)
        w_copy(2, n).wait()
        for m in range(parts):
            got = dot(hid_s[m * rows : (m + 1) * rows, :], wd_s[:, lanes]).astype(BF)
            out_s[m * per : (m + 1) * per, :, lanes] = got.reshape(per, size, ob)
            out_copy(m, n).start()
    for n in range(steps):
        for m in range(parts):
            out_copy(m, n).wait()


def serve_rest_kernel(
    first, parts, x_ref, wg_ref, wu_ref, wd_ref, out_ref, x_s, wd_s, hid_s, out_s, sems, wd_sems, out_sems
):
    srcs, size, model = x_s.shape
    hid = hid_s.shape[1]
    steps = 4
    hb = hid // steps
    ob = model // steps
    per = srcs // parts
    rows = per * size

    def x_copy(m):
        lo = m * per
        return pltpu.make_async_copy(
            x_ref.at[pl.ds(lo, per), pl.ds(first, size), :], x_s.at[pl.ds(lo, per)], sems.at[m]
        )

    def wd_copy(n):
        lanes = pl.ds(n * ob, ob)
        return pltpu.make_async_copy(wd_ref.at[0, :, lanes], wd_s.at[:, lanes], wd_sems.at[n])

    def out_copy(m, n):
        lanes = pl.ds(n * ob, ob)
        return pltpu.make_async_copy(
            out_s.at[pl.ds(m * per, per), :, lanes],
            out_ref.at[pl.ds(m * per, per), :, lanes],
            out_sems.at[m * steps + n],
        )

    for m in range(parts):
        x_copy(m).start()
    for n in range(steps):
        wd_copy(n).start()
    for n in range(steps):
        lanes = slice(n * hb, (n + 1) * hb)
        for m in range(parts):
            if n == 0:
                x_copy(m).wait()
            x = x_s[m * per : (m + 1) * per].reshape(rows, model)
            hidden = silu(dot(x, wg_ref[0, :, lanes])) * dot(x, wu_ref[0, :, lanes])
            hid_s[m * rows : (m + 1) * rows, lanes] = hidden.astype(BF)
    for n in range(steps):
        lanes = slice(n * ob, (n + 1) * ob)
        wd_copy(n).wait()
        for m in range(parts):
            got = dot(hid_s[m * rows : (m + 1) * rows, :], wd_s[:, lanes]).astype(BF)
            out_s[m * per : (m + 1) * per, :, lanes] = got.reshape(per, size, ob)
            out_copy(m, n).start()
    for n in range(steps):
        for m in range(parts):
            out_copy(m, n).wait()


def weights_kernel(main, routes_ref, wt_ref, main_ref, rest_ref):
    tok_rows = routes_ref.shape[1]
    experts = main_ref.shape[1] // main
    routes = jnp.transpose(routes_ref[...])
    wts = jnp.transpose(wt_ref[...])
    lane = lax.broadcasted_iota(jnp.int32, (tok_rows, 128), 1)
    strict = (
        lax.broadcasted_iota(jnp.int32, (tok_rows, tok_rows), 0)
        > lax.broadcasted_iota(jnp.int32, (tok_rows, tok_rows), 1)
    ).astype(BF)
    ones = [lane == routes[:, k : k + 1] for k in range(2)]
    place = dot(strict, jnp.where(ones[0] | ones[1], 1.0, 0.0).astype(BF))
    for ref, base in ((main_ref, 0), (rest_ref, main)):
        size = ref.shape[1] // experts
        j = lax.broadcasted_iota(jnp.int32, ref.shape, 1)
        weight = jnp.zeros(ref.shape, F32)
        for k in range(2):
            p = jnp.sum(jnp.where(ones[k], place, 0.0), axis=1, keepdims=True).astype(jnp.int32)
            p = p - base
            slot = jnp.where((p >= 0) & (p < size), routes[:, k : k + 1] * size + p, -1)
            weight = jnp.where(j == slot, wts[:, k : k + 1], weight)
        ref[...] = weight.astype(BF)


def combine_kernel(main_ref, rest_ref, got_ref, got_rest_ref, upd_ref, out_ref, out_s, sems):
    steps = sems.shape[0]
    blk = out_s.shape[1] // steps

    def out_copy(n):
        lanes = pl.ds(n * blk, blk)
        return pltpu.make_async_copy(out_s.at[:, lanes], out_ref.at[:, lanes], sems.at[n])

    for n in range(steps):
        lanes = slice(n * blk, (n + 1) * blk)
        total = dot(main_ref[...], got_ref[:, lanes]) + dot(rest_ref[...], got_rest_ref[:, lanes])
        out_s[:, lanes] = (upd_ref[:, lanes].astype(F32) + total).astype(out_s.dtype)
        out_copy(n).start()
    for n in range(steps):
        out_copy(n).wait()


def cost(us):
    return pl.CostEstimate(flops=int(us * 5e8), bytes_accessed=int(us * 1e6), transcendentals=0)


def ring(n, size=4):
    return [(i, (i + n) % size) for i in range(size)]


def per_device(
    query_weight,
    forget_preactivation,
    written_input,
    output_gate_logit,
    forget_floor,
    extra_log_decay,
    residual,
    output_weight,
    norm_scale_vector,
    expert_gate_weight,
    expert_up_weight,
    expert_down_weight,
    routes,
    routing_weight,
):
    _, tok, width = query_weight.shape
    model = output_weight.shape[1]
    heads = width // CH
    groups = width // GL
    experts = lax.axis_size(SP)
    cap = 4 * tok // experts
    main = cap * 5 // 6
    rest = cap - main
    z = lax.axis_index("sp_0")
    y = lax.axis_index("sp_1")
    x = lax.axis_index("x")
    core = lax.axis_index("c")

    spikes = lax.dynamic_slice_in_dim(extra_log_decay[0].T, lax.axis_index(SP) * tok, tok, 1)
    q, f, v, gate = (
        a.reshape(tok, width)
        for a in (query_weight, forget_preactivation, written_input, output_gate_logit)
    )
    floor = forget_floor.reshape(1, width)
    scale = norm_scale_vector.reshape(1, model)
    res = residual.reshape(tok, model)

    mine = output_weight
    wmine = [lax.ppermute(mine, "x", ring(n)) for n in (1, 2, 3)]

    tall = pl.BlockSpec((tok, GL), lambda g: (0, g))
    flat = pl.BlockSpec((1, GL), lambda g: (0, g))
    whole = pl.BlockSpec((heads, tok), lambda g: (0, 0))
    pack = pl.pallas_call(
        states_kernel,
        grid=(groups,),
        in_specs=[tall, tall, flat, whole],
        out_specs=pl.BlockSpec((PACK, GL), lambda g: (0, g)),
        out_shape=jax.ShapeDtypeStruct((PACK, width), BF),
        cost_estimate=cost(7),
        compiler_params=pltpu.CompilerParams(vmem_limit_bytes=66 * 1000 * 1000),
        name="states",
    )(f, v, floor, spikes)

    along_y = [lax.ppermute(pack, "sp_1", ring(n)) for n in (1, 2, 3)]


    vm = pl.BlockSpec(memory_space=pltpu.VMEM)
    sm = pl.BlockSpec(memory_space=pltpu.SMEM)

    inside, qrun = pl.pallas_call(
        inside_kernel,
        grid=(groups,),
        in_specs=[tall, tall, tall, flat, whole],
        out_specs=[tall, tall],
        out_shape=[jax.ShapeDtypeStruct((tok, width), F32), jax.ShapeDtypeStruct((tok, width), BF)],
        cost_estimate=cost(8),
        compiler_params=pltpu.CompilerParams(vmem_limit_bytes=66 * 1000 * 1000),
        name="inside",
    )(q, f, v, floor, spikes)

    row, before, btot = pl.pallas_call(
        row_kernel,
        in_specs=[sm, vm, vm, vm, vm],
        out_specs=[vm, vm, vm],
        out_shape=[
            jax.ShapeDtypeStruct((PACK, width), BF),
            jax.ShapeDtypeStruct((CH, width), F32),
            jax.ShapeDtypeStruct((8, width), F32),
        ],
        cost_estimate=cost(2),
        compiler_params=pltpu.CompilerParams(vmem_limit_bytes=66 * 1000 * 1000),
        name="row",
    )(y.astype(jnp.int32).reshape(1), pack, *along_y)

    along_z = [lax.ppermute(row, "sp_0", ring(n)[: 4 - n]) for n in (1, 2, 3)]

    wmine, row = lax.optimization_barrier((wmine, row))
    wmine = [mine] + wmine
    wother = [lax.ppermute(p, "c", ring(1, 2)) for p in wmine]

    route_rows = jnp.pad(routes[0].T, ((0, 6), (0, 0)), constant_values=-1)
    wt_rows = jnp.pad(routing_weight[0].T, ((0, 6), (0, 0)))
    route_rows, wt_rows, row = lax.optimization_barrier((route_rows, wt_rows, row))
    weights_main, weights_rest = pl.pallas_call(
        functools.partial(weights_kernel, main),
        in_specs=[vm, vm],
        out_specs=[vm, vm],
        out_shape=[
            jax.ShapeDtypeStruct((tok, experts * main), BF),
            jax.ShapeDtypeStruct((tok, experts * rest), BF),
        ],
        cost_estimate=cost(2),
        compiler_params=pltpu.CompilerParams(vmem_limit_bytes=66 * 1000 * 1000),
        name="weights",
    )(route_rows, wt_rows)


    place = jnp.stack([z, x, core]).astype(jnp.int32)
    tok_steps = 2
    rows = tok // tok_steps
    send_steps = 4
    send_rows = experts * cap // send_steps
    clip = lambda i: jnp.minimum(i, tok_steps - 1)
    tok_w = pl.BlockSpec((rows, width), lambda i: (clip(i), 0))
    tok_m = pl.BlockSpec((rows, model), lambda i: (clip(i), 0))
    full = lambda a: pl.BlockSpec(a.shape, lambda i: (0,) * a.ndim)


    updated, send = pl.pallas_call(
        functools.partial(mix_kernel, tok_steps, cap),
        grid=(tok_steps + send_steps,),
        in_specs=[
            sm,
            tok_w,
            tok_w,
            tok_w,
            tok_m,
            full(before),
            full(btot),
            full(row),
            full(row),
            full(row),
            *[pl.BlockSpec(memory_space=pl.ANY)] * 8,
            full(scale),
            full(route_rows),
        ],
        out_specs=[
            tok_m,
            pl.BlockSpec((send_rows, model), lambda i: (jnp.maximum(i - tok_steps, 0), 0)),
        ],
        out_shape=[
            jax.ShapeDtypeStruct((tok, model), BF),
            jax.ShapeDtypeStruct((experts * cap, model), BF),
        ],
        scratch_shapes=[
            pltpu.VMEM((width, model), BF),
            pltpu.VMEM((groups, GL, GL), BF),
            pltpu.VMEM((tok, model), BF),
            pltpu.VMEM((experts, tok), jnp.int32),
            pltpu.SemaphoreType.DMA((8,)),
        ],
        compiler_params=pltpu.CompilerParams(vmem_limit_bytes=66 * 1000 * 1000),
        cost_estimate=cost(12),
        name="mix",
    )(place, inside, qrun, gate, res, before, btot, *along_z, *wmine, *wother, scale, route_rows)

    def exchange(a):
        return lax.all_to_all(a, SP, split_axis=0, concat_axis=0, tiled=True)

    hid = expert_gate_weight.shape[2]
    anywhere = pl.BlockSpec(memory_space=pl.ANY)

    dma = lambda n: pltpu.SemaphoreType.DMA((n,))

    def serve(kernel, arrived, first, size, parts, scratch, specs, limit, us):
        return pl.pallas_call(
            functools.partial(kernel, first, parts),
            in_specs=[anywhere, *specs],
            out_specs=anywhere,
            out_shape=jax.ShapeDtypeStruct((experts, size, model), BF),
            scratch_shapes=[
                pltpu.VMEM((experts, size, model), BF),
                *[pltpu.VMEM(shape, BF) for shape in scratch],
                pltpu.VMEM((experts * size, hid), BF),
                pltpu.VMEM((experts, size, model), BF),
                *([dma(parts), dma(4)] if kernel is serve_rest_kernel else [dma(parts + 12)]),
                dma(parts * 4),
            ],
            compiler_params=pltpu.CompilerParams(vmem_limit_bytes=limit * 1024 * 1024),
            cost_estimate=cost(us),
            name="serve",
        )(arrived, expert_gate_weight, expert_up_weight, expert_down_weight)

    def serve_main(arrived):
        scratch = [(model, hid), (model, hid), (hid, model)]
        return serve(serve_kernel, arrived, 0, main, 2, scratch, [anywhere] * 3, 50, 20)

    def serve_rest(arrived):
        specs = [vm, vm, anywhere]
        return serve(serve_rest_kernel, arrived, main, rest, 1, [(hid, model)], specs, 36, 5)

    arrived = exchange(send.reshape(experts, cap, model))
    served_rest = serve_rest(arrived)
    got_rest = exchange(served_rest)

    got = exchange(serve_main(arrived))

    layer_out = pl.pallas_call(
        combine_kernel,
        in_specs=[vm] * 5,
        out_specs=anywhere,
        out_shape=jax.ShapeDtypeStruct((tok, model), BF),
        scratch_shapes=[pltpu.VMEM((tok, model), BF), pltpu.SemaphoreType.DMA((4,))],
        compiler_params=pltpu.CompilerParams(vmem_limit_bytes=40 * 1024 * 1024),
        cost_estimate=cost(4),
        name="combine",
    )(
        weights_main,
        weights_rest,
        got.reshape(experts * main, model),
        got_rest.reshape(experts * rest, model),
        updated,
    )
    return layer_out.reshape(1, tok, model)


def solution(mesh):
    torus = Mesh(
        mesh.devices.reshape(4, 4, 4, mesh.shape["dp"] // 4), ("sp_0", "sp_1", "x", "c")
    )
    return jax.shard_map(
        per_device,
        mesh=torus,
        in_specs=(
            P(DP, SP, None),
            P(DP, SP, None),
            P(DP, SP, None),
            P(DP, SP, None),
            P(),
            P(DP, None, None),
            P(DP, SP, None),
            P(DP, None),
            P(),
            P(SP, None, None),
            P(SP, None, None),
            P(SP, None, None),
            P(DP, SP, None),
            P(DP, SP, None),
        ),
        out_specs=P(DP, SP, None),
        check_vma=False,
    )
```
